32 devices in a mesh: sp: 16 (over z, x, core), tp: 2 (over y).
Axes of the slice: x: 2, y: 2, z: 4, core: 2. Of those that a mesh axis runs over, the one named last changes fastest.
Arguments:
- queries: bfloat16 [10240, 1024], P('sp', 'tp'), may hold values from -160 to 160
- keys: bfloat16 [10240, 256], P('sp', 'tp'), may hold values from -24 to 24
- values: bfloat16 [10240, 256], P('sp', 'tp'), may hold values from -6 to 6
- documents: int32 [10240], P('sp'), may hold values from 0 to 3, never falling along the last dimension, each value on 1 to 5120 neighbouring positions
- sinks: float32 [16], P('tp'), may hold values from -1 to 4
- out_weight: bfloat16 [1024, 2048], replicated, may hold values from -0.1875 to 0.1875
- residual: bfloat16 [10240, 2048], P(('sp', 'tp')), may hold values from -3 to 3
- norm_gain: float32 [2048], replicated, may hold values from 0.1 to 1.9
- up_weight: bfloat16 [2048, 8192], P('sp', 'tp'), may hold values from -0.125 to 0.125
- down_weight: bfloat16 [8192, 2048], P('tp', 'sp'), may hold values from -0.0625 to 0.0625
Outputs:
- layer_out: bfloat16 [10240, 2048], P(('sp', 'tp'))
The draws below stay inside these ranges and needn't reach their ends.
Inputs may be any that keep to these rules, and one draw needn't show every extreme that they name: `documents`: document numbers never fall along the positions; each document holds at most 5120 positions.
All inputs are finite; a program needn't handle non-finite values.
Results may differ from the reference program's by a relative error of at most 0.0095.
Values may be sent and summed in bfloat16 or wider, within the bound.
A program may use at most 128 MiB of HBM per device.

```python
import math
import jax
import jax.numpy as jnp
import numpy as np
from jax import lax

D = 2048
QUERY_HEADS = 16
KEY_VALUE_HEADS = 4
HEAD_SIZE = 64
FF = 8192
WINDOW_REACH = 128
TOK_DEV = 640
PACK_TOKENS = 10240
ATTN = 1024
FF_DEV = 4096
DOCS = 4
N_SP = 16
N_TP = 2


def drawn(key):
    starting_keys = jax.random.normal(jax.random.fold_in(key, 11), (PACK_TOKENS, KEY_VALUE_HEADS, HEAD_SIZE), jnp.float32)
    base_queries = jax.random.normal(jax.random.fold_in(key, 12), (PACK_TOKENS, QUERY_HEADS, HEAD_SIZE), jnp.float32)
    output_keys = starting_keys
    output_queries = base_queries
    return (output_queries.reshape(PACK_TOKENS, QUERY_HEADS * HEAD_SIZE).astype(jnp.bfloat16), output_keys.reshape(PACK_TOKENS, KEY_VALUE_HEADS * HEAD_SIZE).astype(jnp.bfloat16))


def draw_queries(key, part):
    return drawn(key)[0]


def draw_keys(key, part):
    return drawn(key)[1]


def shard_levels(stream_key, dims, cuts, low, largest):
    level = 1.0
    for dim, blocks in cuts:
        heights = jax.random.uniform(jax.random.fold_in(jax.random.fold_in(stream_key, 6), dim), (blocks,), jnp.float32, low / len(cuts), largest / len(cuts))
        level = level * jnp.repeat(jnp.exp(heights), dims[dim] // blocks).reshape((-1,) + (1,) * (len(dims) - 1 - dim))
    return level


def split_up(count, total, limit, lean):
    loads = [(1 << 20) // math.isqrt(grade ** lean) + 1 for grade in range(2, count + 1)]
    surplus, counts = total - limit - (count - 1), [1] * (count - 1)
    while surplus > 0:
        free = [i for i in range(count - 1) if counts[i] < limit]
        mass, budget = sum([loads[i] for i in free]), surplus
        for i in free:
            more = min(limit - counts[i], max(1, budget * loads[i] // mass), surplus)
            counts[i] = counts[i] + more
            surplus = surplus - more
    return np.array([limit] + counts)


def ragged(rng, amount, total, limit, lean):
    if amount == 2:
        one = jax.random.randint(rng, (), max(1, total - limit), min(limit, total - 1) + 1)
        return jnp.stack([one, total - one])
    lengths = jnp.asarray(split_up(amount, total, limit, lean), jnp.int32)
    couples = (amount - 1) // 2
    giver, taker = lengths[1:1 + 2 * couples:2], lengths[2:2 + 2 * couples:2]
    margin = jnp.minimum(giver - 1, limit - taker)
    shifted = jax.random.randint(jax.random.fold_in(rng, 1), (couples,), 0, 1 << 20) % (margin + 1)
    lengths = lengths.at[1:1 + 2 * couples:2].set(giver - shifted).at[2:2 + 2 * couples:2].set(taker + shifted)
    return lengths[jax.random.permutation(jax.random.fold_in(rng, 2), amount)]


def noise(own_key, shape, spread, bound, pieces=(), kind=jnp.bfloat16):
    array = jax.random.normal(own_key, shape, jnp.float32) * spread
    if len(pieces) > 0:
        array = shard_levels(own_key, shape, pieces, -0.22, 0.18) * array
    return jnp.clip(array, min=-bound, max=bound).astype(kind)


def setup_inputs(seed: int = 0) -> dict:
    streams_of = jax.random.split(jax.random.key(seed), 11)
    queries = draw_queries(jax.random.fold_in(streams_of[10], 71), 0)
    keys = draw_keys(jax.random.fold_in(streams_of[10], 71), 0)
    values = noise(streams_of[2], (PACK_TOKENS, KEY_VALUE_HEADS * HEAD_SIZE), 1.0, 6.0, ((0, 16), (1, 2)))
    documents = jnp.searchsorted(jnp.cumsum(ragged(streams_of[3], DOCS, PACK_TOKENS, 8 * TOK_DEV, 1)), jnp.arange(PACK_TOKENS), side="right").astype(jnp.int32)
    sinks = jnp.clip(-1.0 + 5.0 * jax.random.uniform(streams_of[4], (QUERY_HEADS,), jnp.float32) ** shard_levels(streams_of[4], (QUERY_HEADS,), ((0, 2),), -0.2, 0.2), -1.0, 4.0)
    out_weight = noise(streams_of[5], (ATTN, D), ATTN ** -0.5, 0.1875)
    residual = noise(streams_of[6], (PACK_TOKENS, D), 0.5, 3.0, ((0, 32),))
    norm_gain = jnp.clip(1.0 + 0.18 * jax.random.normal(streams_of[7], (D,), jnp.float32), 0.1, 1.9)
    up_weight = noise(streams_of[8], (D, FF), D ** -0.5, 0.125, ((0, 16), (1, 2)))
    down_weight = noise(streams_of[9], (FF, D), FF ** -0.5, 0.0625, ((0, 2), (1, 16)))
    return {"queries": queries, "keys": keys, "values": values, "documents": documents, "sinks": sinks, "out_weight": out_weight, "residual": residual, "norm_gain": norm_gain, "up_weight": up_weight, "down_weight": down_weight}


masked_score = -1e+30
epsilon = 1e-06

def rounded(value):
    return lax.optimization_barrier(value.astype(jnp.bfloat16))

def reference(queries, keys, values, documents, sinks, out_weight, residual, norm_gain, up_weight, down_weight):
    query_group = QUERY_HEADS // KEY_VALUE_HEADS
    block_list = PACK_TOKENS // WINDOW_REACH
    key_matrix = jnp.concatenate([jnp.zeros((WINDOW_REACH, KEY_VALUE_HEADS * HEAD_SIZE), jnp.bfloat16), keys], axis=0).reshape(block_list + 1, WINDOW_REACH, KEY_VALUE_HEADS, HEAD_SIZE)
    value_matrix = jnp.concatenate([jnp.zeros((WINDOW_REACH, KEY_VALUE_HEADS * HEAD_SIZE), jnp.bfloat16), values], axis=0).reshape(block_list + 1, WINDOW_REACH, KEY_VALUE_HEADS, HEAD_SIZE)
    doc_ids = documents.astype(jnp.int32)
    key_docs = jnp.concatenate([jnp.full((WINDOW_REACH,), -1, jnp.int32), doc_ids], axis=0).reshape(block_list + 1, WINDOW_REACH)
    query_docs = doc_ids.reshape(block_list, WINDOW_REACH)
    grouped_queries = queries.reshape(block_list, WINDOW_REACH, KEY_VALUE_HEADS, query_group, HEAD_SIZE)
    head_sink_logit = sinks.astype(jnp.float32).reshape(KEY_VALUE_HEADS, query_group, 1)
    row_index = jnp.arange(WINDOW_REACH, dtype=jnp.int32)[:, None]
    col_index = jnp.arange(2 * WINDOW_REACH, dtype=jnp.int32)[None, :]
    distance = WINDOW_REACH + row_index - col_index
    near = (distance >= 0) & (distance < WINDOW_REACH)

    def one_block(items):
        block_queries, early_keys, late_keys, early_values, late_values, early_docs, late_docs, own_docs = items
        band_keys = jnp.concatenate([early_keys, late_keys], axis=0).astype(jnp.float32)
        band_values = jnp.concatenate([early_values, late_values], axis=0).astype(jnp.float32)
        band_docs = jnp.concatenate([early_docs, late_docs], axis=0)
        visible = (near & (band_docs[None, :] == own_docs[:, None]))[None, None]
        scores = jnp.einsum('qhgd,shd->hgqs', block_queries.astype(jnp.float32), band_keys) * HEAD_SIZE ** (-0.5)
        scores = jnp.where(visible, scores, masked_score)
        top = jnp.maximum(lax.optimization_barrier(jnp.max(scores, axis=-1)), head_sink_logit)
        exponent = jnp.where(visible, jnp.exp(scores - top[..., None]), 0.0)
        total = jnp.exp(head_sink_logit - top) + lax.optimization_barrier(jnp.sum(exponent, axis=-1))
        shares = rounded(exponent / total[..., None])
        attended = jnp.einsum('hgqs,shd->qhgd', shares.astype(jnp.float32), band_values)
        return attended.astype(jnp.bfloat16).reshape(WINDOW_REACH, QUERY_HEADS * HEAD_SIZE)
    attended = lax.map(one_block, (grouped_queries, key_matrix[:-1], key_matrix[1:], value_matrix[:-1], value_matrix[1:], key_docs[:-1], key_docs[1:], query_docs))
    attended = attended.reshape(PACK_TOKENS, QUERY_HEADS * HEAD_SIZE)
    projected = jnp.dot(attended.astype(jnp.float32), out_weight.astype(jnp.float32), preferred_element_type=jnp.float32)
    mixed = rounded(residual.astype(jnp.float32) + rounded(projected).astype(jnp.float32))
    widened = mixed.astype(jnp.float32)
    normed = (widened * lax.rsqrt(lax.optimization_barrier(jnp.mean(widened * widened, axis=-1, keepdims=True)) + epsilon) * norm_gain.astype(jnp.float32)).astype(jnp.bfloat16)
    down_groups = down_weight.astype(jnp.float32).reshape(N_TP, FF_DEV, D)

    def mixer_block(rows):
        before = jnp.dot(rows.astype(jnp.float32), up_weight.astype(jnp.float32), preferred_element_type=jnp.float32)
        hidden = jnp.square(jax.nn.relu(before)).astype(jnp.bfloat16)
        parts = jnp.einsum('rnf,nfd->nrd', hidden.reshape(rows.shape[0], N_TP, FF_DEV).astype(jnp.float32), down_groups)
        return lax.optimization_barrier(jnp.sum(rounded(parts).astype(jnp.float32), axis=0))
    branch = lax.map(mixer_block, normed.reshape(N_SP, TOK_DEV, D)).reshape(PACK_TOKENS, D)
    return (widened + rounded(branch).astype(jnp.float32)).astype(jnp.bfloat16)
```

```python
import functools

import jax
import jax.numpy as jnp
from jax import lax
from jax.experimental import pallas as pl
from jax.experimental.pallas import tpu as pltpu
from jax.sharding import PartitionSpec as P

HEAD_SIZE = 64
WINDOW_REACH = 128
LANES = 128
CORES = 2
MESH = pl.DeviceIdType.MESH

masked_score = -1e30
epsilon = 1e-06


def passed_along(shard, axis, by):
    peers = lax.axis_size(axis)
    pairs = [(i, i + by) for i in range(peers) if 0 <= i + by < peers]
    return lax.ppermute(shard, axis, pairs)


def rounded(value):
    return lax.optimization_barrier(value.astype(jnp.bfloat16))


def squared_relu(before):
    return jnp.square(jax.nn.relu(before)).astype(jnp.bfloat16)


def windowed_attention(queries, keys, values, documents, sinks):
    length = queries.shape[0]
    heads = queries.shape[1] // HEAD_SIZE
    kv_heads = keys.shape[1] // HEAD_SIZE
    query_group = heads // kv_heads
    block_list = length // WINDOW_REACH
    prev_keys, prev_values, prev_docs = passed_along(
        (
            keys[length - WINDOW_REACH :],
            values[length - WINDOW_REACH :],
            documents[length - WINDOW_REACH :],
        ),
        "sp",
        1,
    )
    offset = lax.axis_index("sp") * length
    key_matrix = jnp.concatenate([prev_keys, keys], axis=0).reshape(
        block_list + 1, WINDOW_REACH, kv_heads, HEAD_SIZE
    )
    value_matrix = jnp.concatenate([prev_values, values], axis=0).reshape(
        block_list + 1, WINDOW_REACH, kv_heads, HEAD_SIZE
    )
    key_docs = jnp.concatenate([prev_docs, documents], axis=0).reshape(block_list + 1, WINDOW_REACH)
    key_place = (
        offset - WINDOW_REACH + jnp.arange((block_list + 1) * WINDOW_REACH, dtype=jnp.int32)
    ).reshape(block_list + 1, WINDOW_REACH)
    band_keys = jnp.concatenate([key_matrix[:-1], key_matrix[1:]], axis=1)
    band_values = jnp.concatenate([value_matrix[:-1], value_matrix[1:]], axis=1)
    band_docs = jnp.concatenate([key_docs[:-1], key_docs[1:]], axis=1)
    band_place = jnp.concatenate([key_place[:-1], key_place[1:]], axis=1)
    query_docs = documents.reshape(block_list, WINDOW_REACH)
    grouped_queries = queries.reshape(block_list, WINDOW_REACH, kv_heads, query_group, HEAD_SIZE)
    scores = jnp.einsum(
        "nqhgd,nshd->nhgqs", grouped_queries, band_keys, preferred_element_type=jnp.float32
    ) * HEAD_SIZE ** (-0.5)
    row_index = jnp.arange(WINDOW_REACH, dtype=jnp.int32)[:, None]
    col_index = jnp.arange(2 * WINDOW_REACH, dtype=jnp.int32)[None, :]
    distance = WINDOW_REACH + row_index - col_index
    near = (distance >= 0) & (distance < WINDOW_REACH)
    visible = (
        near[None]
        & (band_docs[:, None, :] == query_docs[:, :, None])
        & (band_place[:, None, :] >= 0)
    )
    visible = visible[:, None, None]
    head_sink_logit = sinks.reshape(kv_heads, query_group)[None, :, :, None]
    scores = jnp.where(visible, scores, masked_score)
    top = jnp.maximum(jnp.max(scores, axis=-1), head_sink_logit)
    exponent = jnp.where(visible, jnp.exp(scores - top[..., None]), 0.0)
    total = jnp.exp(head_sink_logit - top) + jnp.sum(exponent, axis=-1)
    shares = (exponent / total[..., None]).astype(jnp.bfloat16)
    attended = jnp.einsum(
        "nhgqs,nshd->nqhgd", shares, band_values, preferred_element_type=jnp.float32
    )
    return attended.astype(jnp.bfloat16).reshape(length, heads * HEAD_SIZE)


def rotated(shard, axis, by):
    peers = lax.axis_size(axis)
    return lax.ppermute(shard, axis, [(i, (i + by) % peers) for i in range(peers)])


def row_block(array, index, rows):
    return lax.dynamic_slice_in_dim(array, index * rows, rows, axis=0)


def gathered_body(
    queries, keys, values, documents, sinks, out_weight, residual, norm_gain, up_weight, down_weight
):
    up_whole, down_whole = (
        lax.all_gather(up_weight, "sp", axis=0, tiled=True),
        lax.all_gather(down_weight, "sp", axis=1, tiled=True),
    )
    n_tp = lax.axis_size("tp")
    me = lax.axis_index("tp")
    rows = residual.shape[0]
    attended = windowed_attention(queries, keys, values, documents, sinks)
    width = attended.shape[1]
    token_heads = jnp.zeros((rows, width * n_tp), jnp.bfloat16)
    for by in range(n_tp):
        piece = row_block(attended, (me + by) % n_tp, rows)
        if by:
            piece = rotated(piece, "tp", by)
        token_heads = lax.dynamic_update_slice_in_dim(
            token_heads, piece, ((me - by) % n_tp) * width, axis=1
        )
    projected = jnp.dot(token_heads, out_weight, preferred_element_type=jnp.float32)
    mixed = rounded(residual.astype(jnp.float32) + rounded(projected).astype(jnp.float32))
    widened = mixed.astype(jnp.float32)
    normed = (
        widened
        * lax.rsqrt(jnp.mean(widened * widened, axis=-1, keepdims=True) + epsilon)
        * norm_gain
    ).astype(jnp.bfloat16)
    branch = 0.0
    for by in range(n_tp - 1, -1, -1):
        rows_in = rotated(normed, "tp", by) if by else normed
        hidden = squared_relu(jnp.dot(rows_in, up_whole, preferred_element_type=jnp.float32))
        partial = jnp.dot(hidden, down_whole, preferred_element_type=jnp.float32).astype(
            jnp.bfloat16
        )
        if by:
            partial = rotated(partial, "tp", n_tp - by)
        branch = branch + partial.astype(jnp.float32)
    return (widened + rounded(branch).astype(jnp.float32)).astype(jnp.bfloat16)


def fits(mesh, tokens, width, kv_width, model, hidden):
    n_sp, n_tp = mesh.shape["sp"], mesh.shape["tp"]
    block = model // n_sp
    return (
        n_tp == 2
        and n_sp % (n_tp * CORES) == 0
        and block % LANES == 0
        and kv_width == LANES
        and width % (2 * LANES) == 0
        and tokens % (2 * WINDOW_REACH // 2) == 0
        and (tokens // n_tp) % 32 == 0
        and hidden % (n_tp * 2 * LANES) == 0
    )


def layer_kernel(
    n_z,
    q_hbm, k_hbm, v_hbm, docs_hbm, sinks, outw_hbm, res_hbm, gain_ref, up_hbm, down_hbm,
    out_hbm,
    up_all, down_all, rows_all, hid_all, outw, res, mixed, q_ref, k_ref, v_ref, docs,
    k_wide, v_wide, att, oth, psend, precv, own_sum, out_ref,
    load_sem, halo_send, halo_recv, xs_sem, z_send, z_recv, d_send, d_recv, y_sem,
    g_send, g_recv, p_send, p_recv, own_sem,
):
    sp, y = lax.axis_index("sp"), lax.axis_index("tp")
    n_x, n_y = 2, 2
    z, x, c = sp // (n_x * CORES), lax.rem(sp // CORES, n_x), lax.rem(sp, CORES)
    n_sp = n_z * n_x * CORES
    tokens = q_ref.shape[0]
    rows = res.shape[0]
    half = rows // 2
    model = res.shape[1]
    width = q_ref.shape[1]
    blk = up_hbm.shape[0]
    quarter = up_hbm.shape[1] // n_x
    wide = 2 * blk

    def at(zz, xx, yy, cc):
        return ((zz * n_x + xx) * CORES + cc, yy)

    def remote(src, dst, send, recv, dev):
        return pltpu.make_async_remote_copy(
            src_ref=src, dst_ref=dst, send_sem=send, recv_sem=recv, device_id=dev, device_id_type=MESH
        )

    x_peer, y_peer, c_peer = at(z, 1 - x, y, c), at(z, x, 1 - y, c), at(z, x, y, 1 - c)

    def block(phase, zb, xb, cb):
        if phase == 0:
            first = ((zb * n_x + xb) * CORES + cb) * blk
            return up_all.at[pl.ds(pl.multiple_of(first, blk), blk), :]
        return down_all.at[zb * n_x + xb, :, pl.ds(pl.multiple_of(cb * blk, blk), blk)]

    def own_piece(phase, xq):
        start = pl.multiple_of(xq * quarter, quarter)
        if phase == 0:
            return up_hbm.at[:, pl.ds(start, quarter)]
        return down_hbm.at[pl.ds(start, quarter), :]

    def x_exchange(phase):
        return remote(
            own_piece(phase, 1 - x), block(phase, z, x, c), xs_sem.at[phase], z_recv.at[phase, z, 1], x_peer
        )

    def own_load(phase):
        return pltpu.make_async_copy(own_piece(phase, x), block(phase, z, x, c), own_sem.at[phase])

    low = jnp.minimum(z, n_z - 1 - z)

    def plane(k):
        near = jnp.where(lax.rem(k, 2) == 1, z - (k + 1) // 2, z + (k + 1) // 2)
        far = jnp.where(z < n_z - 1 - z, k, n_z - 1 - k)
        return jnp.where(k <= 2 * low, near, far)

    def place(t):
        zb, b = plane(t // 2), lax.rem(t, 2)
        return zb, b, jnp.where(b == 0, x, 1 - x)

    def to_up(phase, zb, b, xb):
        ref = block(phase, zb, xb, c)
        return remote(ref, ref, z_send.at[0, phase, zb, b], z_recv.at[phase, zb, b], at(z + 1, x, y, c))

    def to_down(phase, zb, b, xb):
        ref = block(phase, zb, xb, c)
        return remote(ref, ref, z_send.at[1, phase, zb, b], z_recv.at[phase, zb, b], at(z - 1, x, y, c))

    def to_core(phase, zb, b, xb):
        ref = block(phase, zb, xb, c)
        return remote(ref, ref, d_send.at[phase, zb, b], d_recv.at[phase, zb, b], c_peer)

    def goes_up(zb):
        return jnp.logical_and(zb <= z, z < n_z - 1)

    def goes_down(zb):
        return jnp.logical_and(zb >= z, z > 0)

    def pass_on(phase, t):
        zb, b, xb = place(t)

        @pl.when(goes_up(zb))
        def _():
            to_up(phase, zb, b, xb).start()

        @pl.when(goes_down(zb))
        def _():
            to_down(phase, zb, b, xb).start()

        to_core(phase, zb, b, xb).start()

    def arrive(phase, t):
        zb, b, xb = place(t)
        to_up(phase, zb, b, xb).wait_recv()
        pass_on(phase, t)

    last = tokens - WINDOW_REACH
    nxt = (sp + 1, y)

    def halo(i):
        src, dst = (
            (k_hbm.at[pl.ds(last, WINDOW_REACH), :], k_ref.at[pl.ds(0, WINDOW_REACH), :]),
            (v_hbm.at[pl.ds(last, WINDOW_REACH), :], v_ref.at[pl.ds(0, WINDOW_REACH), :]),
            (docs_hbm.at[last // LANES], docs.at[0]),
        )[i]
        return remote(src, dst, halo_send.at[i], halo_recv.at[i], nxt)

    @pl.when(sp < n_sp - 1)
    def _():
        for i in range(3):
            halo(i).start()

    own_load(0).start()
    loads = [
        pltpu.make_async_copy(q_hbm, q_ref, load_sem.at[0]),
        pltpu.make_async_copy(k_hbm, k_ref.at[pl.ds(WINDOW_REACH, tokens), :], load_sem.at[1]),
        pltpu.make_async_copy(v_hbm, v_ref.at[pl.ds(WINDOW_REACH, tokens), :], load_sem.at[2]),
        pltpu.make_async_copy(docs_hbm, docs.at[pl.ds(1, tokens // LANES)], load_sem.at[3]),
        pltpu.make_async_copy(outw_hbm, outw, load_sem.at[4]),
        pltpu.make_async_copy(res_hbm, res, load_sem.at[5]),
    ]
    x_exchange(0).start()
    own_load(0).wait()
    pass_on(0, 0)
    for load in loads:
        load.start()
    own_load(1).start()
    x_exchange(1).start()

    @pl.when(sp == 0)
    def _():
        k_ref[pl.ds(0, WINDOW_REACH), :] = jnp.zeros((WINDOW_REACH, LANES), jnp.bfloat16)
        v_ref[pl.ds(0, WINDOW_REACH), :] = jnp.zeros((WINDOW_REACH, LANES), jnp.bfloat16)
        docs[0] = jnp.full(docs.shape[1:], -1, jnp.int32)

    for load in loads[:4]:
        load.wait()

    @pl.when(sp > 0)
    def _():
        for i in range(3):
            halo(i).wait_recv()

    heads = width // HEAD_SIZE
    kv_heads = LANES // HEAD_SIZE
    group = heads // kv_heads
    lane_in = lax.broadcasted_iota(jnp.int32, (LANES, LANES), 0)
    lane_out = lax.broadcasted_iota(jnp.int32, (LANES, LANES), 1)
    for g in range(kv_heads):
        for par in range(2):
            pick = (lane_in - g * HEAD_SIZE == lane_out - par * HEAD_SIZE) & (
                lane_out // HEAD_SIZE == par
            )
            pick = pick.astype(jnp.float32).astype(jnp.bfloat16)
            for raw, spread in ((k_ref, k_wide), (v_ref, v_wide)):
                spread[g * 2 + par] = jnp.dot(
                    raw[...], pick, preferred_element_type=jnp.float32
                ).astype(jnp.bfloat16)

    row_i = lax.broadcasted_iota(jnp.int32, (WINDOW_REACH, 2 * WINDOW_REACH), 0)
    col_i = lax.broadcasted_iota(jnp.int32, (WINDOW_REACH, 2 * WINDOW_REACH), 1)
    near = (col_i > row_i) & (col_i <= row_i + WINDOW_REACH)

    def attend(n, carry):
        start = pl.multiple_of(n * WINDOW_REACH, WINDOW_REACH)
        early = jnp.broadcast_to(docs[n], (WINDOW_REACH, LANES))
        late = jnp.broadcast_to(docs[n + 1], (WINDOW_REACH, LANES))
        mine = late.T
        same = jnp.concatenate([early == mine, late == mine], axis=1)
        visible = near & same
        for j in range(width // LANES):
            total_out = None
            g = (2 * j) // group
            q_blk = q_ref[pl.ds(start, WINDOW_REACH), j * LANES : (j + 1) * LANES]
            for par in range(2):
                head = 2 * j + par
                keys = k_wide[g * 2 + par, pl.ds(start, 2 * WINDOW_REACH), :]
                vals = v_wide[g * 2 + par, pl.ds(start, 2 * WINDOW_REACH), :]
                scores = lax.dot_general(
                    q_blk, keys, (((1,), (1,)), ((), ())), preferred_element_type=jnp.float32
                ) * HEAD_SIZE ** (-0.5)
                scores = jnp.where(visible, scores, masked_score)
                sink = sinks[head]
                top = jnp.maximum(jnp.max(scores, axis=1, keepdims=True), sink)
                exponent = jnp.where(visible, jnp.exp(scores - top), 0.0)
                total = jnp.exp(sink - top) + jnp.sum(exponent, axis=1, keepdims=True)
                shares = (exponent * (1.0 / total)).astype(jnp.bfloat16)
                part = jnp.dot(shares, vals, preferred_element_type=jnp.float32)
                total_out = part if total_out is None else total_out + part
            att[pl.ds(start, WINDOW_REACH), j * LANES : (j + 1) * LANES] = total_out.astype(
                jnp.bfloat16
            )
        return carry

    lax.fori_loop(0, tokens // WINDOW_REACH, attend, 0)

    mine_at = pl.multiple_of(y * rows, rows)
    theirs_at = pl.multiple_of((1 - y) * rows, rows)
    swap = remote(att.at[pl.ds(theirs_at, rows), :], oth, y_sem.at[0], y_sem.at[1], y_peer)
    swap.start()
    arrive(0, 1)
    arrive(0, 2)
    loads[4].wait()
    loads[5].wait()
    swap.wait_recv()

    me_p = x * n_y + y
    x_p, y_p, d_p = (1 - x) * n_y + y, x * n_y + 1 - y, (1 - x) * n_y + 1 - y
    chunk = 2 * wide

    def row_part(p, h):
        return rows_all.at[pl.ds(pl.multiple_of(p * rows + h * half, half), half), :]

    def give(p, h, way):
        slot = p * 2 + h
        ref = row_part(p, h)
        return remote(ref, ref, g_send.at[way, slot], g_recv.at[slot], x_peer if way == 0 else y_peer)

    for h in range(2):
        own_rows = pl.ds(pl.multiple_of(mine_at + h * half, half), half)

        def project(n, square):
            cols = pl.ds(pl.multiple_of(n * chunk, chunk), chunk)
            acc = jnp.dot(
                att[own_rows, :], outw[pl.ds(pl.multiple_of(y * width, width), width), cols],
                preferred_element_type=jnp.float32,
            ) + jnp.dot(
                oth[h * half : (h + 1) * half, :],
                outw[pl.ds(pl.multiple_of((1 - y) * width, width), width), cols],
                preferred_element_type=jnp.float32,
            )
            sums = res[h * half : (h + 1) * half, cols].astype(jnp.float32) + acc.astype(
                jnp.bfloat16
            ).astype(jnp.float32)
            sums = sums.astype(jnp.bfloat16)
            mixed[h * half : (h + 1) * half, cols] = sums
            sums = sums.astype(jnp.float32)
            return square + jnp.sum(sums * sums, axis=1, keepdims=True)

        square = lax.fori_loop(0, model // chunk, project, jnp.zeros((half, 1), jnp.float32))
        scale = lax.rsqrt(square * (1.0 / model) + epsilon)

        def normalise(n, carry):
            cols = pl.ds(pl.multiple_of(n * chunk, chunk), chunk)
            wide_rows = mixed[h * half : (h + 1) * half, cols].astype(jnp.float32)
            rows_all[pl.ds(pl.multiple_of(me_p * rows + h * half, half), half), cols] = (
                wide_rows * scale * gain_ref[:, cols]
            ).astype(jnp.bfloat16)
            return carry

        lax.fori_loop(0, model // chunk, normalise, 0)
        give(me_p, h, 0).start()
        give(me_p, h, 1).start()

    arrive(0, 3)
    n_items = 2 * n_z

    def more(first, until):
        for t in range(first, min(until, n_items)):
            arrive(0, t)

    more(4, 6)
    give(x_p, 0, 0).wait_recv()
    give(x_p, 0, 1).start()
    more(6, 7)
    give(y_p, 1, 1).wait_recv()
    give(y_p, 1, 0).start()
    more(7, n_items)

    own_load(1).wait()
    pass_on(1, 0)
    arrive(1, 1)

    give(x_p, 1, 0).wait_recv()
    give(y_p, 0, 1).wait_recv()
    give(d_p, 0, 1).wait_recv()
    give(d_p, 1, 0).wait_recv()

    def core_wait(phase):
        def wait_one(t, carry):
            zb, b, xb = place(t)
            to_core(phase, zb, b, xb).wait_recv()
            return carry
        return wait_one

    lax.fori_loop(0, n_items, core_wait(0), 0)
    tall = 2 * rows

    def up_step(i, carry):
        r = pl.ds(pl.multiple_of((i // (quarter // chunk)) * tall, tall), tall)
        f = pl.ds(pl.multiple_of(lax.rem(i, quarter // chunk) * chunk, chunk), chunk)
        before = jnp.dot(rows_all[r, :], up_all[:, f], preferred_element_type=jnp.float32)
        before = jnp.maximum(before, 0.0)
        hid_all[r, f] = (before * before).astype(jnp.bfloat16)
        return carry

    lax.fori_loop(0, 2 * (quarter // chunk), up_step, 0)

    def partial_copy(j, s):
        px, py = jnp.where(s >= 2, 1 - x, x), jnp.where(lax.rem(s, 2) == 1, 1 - y, y)
        return remote(
            psend.at[j, s - 1], precv.at[j, s - 1], p_send.at[j, s - 1], p_recv.at[j, s - 1], at(z, px, py, c)
        )

    def combine(t):
        zb, b, xb = place(t)
        j = zb * n_x + xb
        total = own_sum[j]
        for s in (1, 2, 3):
            partial_copy(j, s).wait_recv()
            total = total + precv[j, s - 1].astype(jnp.float32)
        cols = pl.ds(pl.multiple_of(j * wide, wide), wide)
        out_ref[:, cols] = (
            mixed[:, cols].astype(jnp.float32) + total.astype(jnp.bfloat16).astype(jnp.float32)
        ).astype(jnp.bfloat16)

    def down_step(t, carry):
        @pl.when(t >= 2)
        def _():
            arrive(1, t)

        zb, b, xb = place(t)
        to_core(1, zb, b, xb).wait_recv()
        j = zb * n_x + xb

        def piece(i, carry):
            s = 3 - i
            px, py = jnp.where(s >= 2, 1 - x, x), jnp.where(lax.rem(s, 2) == 1, 1 - y, y)
            first = pl.multiple_of((px * n_y + py) * rows, rows)
            part = jnp.dot(
                hid_all[pl.ds(first, rows), :], down_all[j], preferred_element_type=jnp.float32
            )

            @pl.when(s > 0)
            def _():
                psend[j, s - 1] = part.astype(jnp.bfloat16)
                partial_copy(j, s).start()

            @pl.when(s == 0)
            def _():
                own_sum[j] = part

            return carry

        lax.fori_loop(0, n_x * n_y, piece, 0)

        @pl.when(t >= 2)
        def _():
            combine(t - 2)

        return carry

    lax.fori_loop(0, n_items, down_step, 0)
    for t in (n_items - 2, n_items - 1):
        combine(jnp.int32(t))
    store = pltpu.make_async_copy(out_ref, out_hbm, load_sem.at[0])
    store.start()

    @pl.when(sp < n_sp - 1)
    def _():
        for i in range(3):
            halo(i).wait_send()

    swap.wait_send()
    for phase in range(2):
        x_exchange(phase).wait_send()
    for h in range(2):
        give(me_p, h, 0).wait_send()
        give(me_p, h, 1).wait_send()
    give(x_p, 0, 1).wait_send()
    give(y_p, 1, 0).wait_send()

    def sent(t, carry):
        zb, b, xb = place(t)
        for phase in range(2):
            @pl.when(goes_up(zb))
            def _():
                to_up(phase, zb, b, xb).wait_send()

            @pl.when(goes_down(zb))
            def _():
                to_down(phase, zb, b, xb).wait_send()

            to_core(phase, zb, b, xb).wait_send()
        for s in (1, 2, 3):
            partial_copy(zb * n_x + xb, s).wait_send()
        return carry

    lax.fori_loop(0, n_items, sent, 0)
    store.wait()


def kernel_body(
    n_z, queries, keys, values, documents, sinks, out_weight, residual, norm_gain, up_weight, down_weight
):
    tokens, width = queries.shape
    rows, model = residual.shape
    blk, hidden = up_weight.shape
    quarter = hidden // 2
    group = 4 * rows
    pairs = 2 * n_z
    bf16, f32 = jnp.bfloat16, jnp.float32
    hbm = pl.BlockSpec(memory_space=pl.ANY)
    dma = pltpu.SemaphoreType.DMA
    return pl.pallas_call(
        functools.partial(layer_kernel, n_z),
        out_shape=jax.ShapeDtypeStruct((rows, model), bf16),
        in_specs=[hbm, hbm, hbm, hbm, pl.BlockSpec(memory_space=pltpu.SMEM), hbm, hbm,
                  pl.BlockSpec(memory_space=pltpu.VMEM), hbm, hbm],
        out_specs=hbm,
        scratch_shapes=[
            pltpu.VMEM((model, quarter), bf16),
            pltpu.VMEM((pairs, quarter, 2 * blk), bf16),
            pltpu.VMEM((group, model), bf16),
            pltpu.VMEM((group, quarter), bf16),
            pltpu.VMEM(out_weight.shape, bf16),
            pltpu.VMEM((rows, model), bf16),
            pltpu.VMEM((rows, model), bf16),
            pltpu.VMEM((tokens, width), bf16),
            pltpu.VMEM((tokens + WINDOW_REACH, LANES), bf16),
            pltpu.VMEM((tokens + WINDOW_REACH, LANES), bf16),
            pltpu.VMEM((tokens // LANES + 1, 1, LANES), jnp.int32),
            pltpu.VMEM((4, tokens + WINDOW_REACH, LANES), bf16),
            pltpu.VMEM((4, tokens + WINDOW_REACH, LANES), bf16),
            pltpu.VMEM((tokens, width), bf16),
            pltpu.VMEM((rows, width), bf16),
            pltpu.VMEM((pairs, 3, rows, 2 * blk), bf16),
            pltpu.VMEM((pairs, 3, rows, 2 * blk), bf16),
            pltpu.VMEM((pairs, rows, 2 * blk), f32),
            pltpu.VMEM((rows, model), bf16),
            dma((6,)), dma((3,)), dma((3,)), dma((2,)), dma((2, 2, n_z, 2)), dma((2, n_z, 2)),
            dma((2, n_z, 2)), dma((2, n_z, 2)), dma((2,)), dma((2, 8)), dma((8,)),
            dma((pairs, 3)), dma((pairs, 3)), dma((2,)),
        ],
        compiler_params=pltpu.CompilerParams(has_side_effects=True, vmem_limit_bytes=67043328),
    )(
        queries, keys, values, documents.reshape(tokens // LANES, 1, LANES), sinks, out_weight,
        residual, norm_gain.reshape(1, model), up_weight, down_weight,
    )


def body(n_z, mesh, *arrays):
    queries, keys, up_weight, residual = arrays[0], arrays[1], arrays[8], arrays[6]
    if fits(mesh, *queries.shape, keys.shape[1], residual.shape[1], up_weight.shape[1]):
        return kernel_body(n_z, *arrays)
    return gathered_body(*arrays)


def solution(mesh):
    in_specs = (
        P("sp", "tp"),
        P("sp", "tp"),
        P("sp", "tp"),
        P("sp"),
        P("tp"),
        P(),
        P(("sp", "tp"), None),
        P(),
        P("sp", "tp"),
        P("tp", "sp"),
    )
    out_specs = P(("sp", "tp"), None)
    n_z = mesh.shape["sp"] // (CORES * mesh.shape["tp"])
    return jax.shard_map(
        functools.partial(body, n_z, mesh), mesh=mesh, in_specs=in_specs, out_specs=out_specs, check_vma=False
    )
```

```python
import functools

import jax
import jax.numpy as jnp
from jax import lax
from jax.experimental import pallas as pl
from jax.experimental.pallas import tpu as pltpu
from jax.sharding import PartitionSpec as P

HEAD_SIZE = 64
WINDOW_REACH = 128
LANES = 128
CORES = 2
MESH = pl.DeviceIdType.MESH

masked_score = -1e30
epsilon = 1e-06


def passed_along(shard, axis, by):
    peers = lax.axis_size(axis)
    pairs = [(i, i + by) for i in range(peers) if 0 <= i + by < peers]
    return lax.ppermute(shard, axis, pairs)


def rounded(value):
    return lax.optimization_barrier(value.astype(jnp.bfloat16))


def squared_relu(before):
    return jnp.square(jax.nn.relu(before)).astype(jnp.bfloat16)


def windowed_attention(queries, keys, values, documents, sinks):
    length = queries.shape[0]
    heads = queries.shape[1] // HEAD_SIZE
    kv_heads = keys.shape[1] // HEAD_SIZE
    query_group = heads // kv_heads
    block_list = length // WINDOW_REACH
    prev_keys, prev_values, prev_docs = passed_along(
        (
            keys[length - WINDOW_REACH :],
            values[length - WINDOW_REACH :],
            documents[length - WINDOW_REACH :],
        ),
        "sp",
        1,
    )
    offset = lax.axis_index("sp") * length
    key_matrix = jnp.concatenate([prev_keys, keys], axis=0).reshape(
        block_list + 1, WINDOW_REACH, kv_heads, HEAD_SIZE
    )
    value_matrix = jnp.concatenate([prev_values, values], axis=0).reshape(
        block_list + 1, WINDOW_REACH, kv_heads, HEAD_SIZE
    )
    key_docs = jnp.concatenate([prev_docs, documents], axis=0).reshape(block_list + 1, WINDOW_REACH)
    key_place = (
        offset - WINDOW_REACH + jnp.arange((block_list + 1) * WINDOW_REACH, dtype=jnp.int32)
    ).reshape(block_list + 1, WINDOW_REACH)
    band_keys = jnp.concatenate([key_matrix[:-1], key_matrix[1:]], axis=1)
    band_values = jnp.concatenate([value_matrix[:-1], value_matrix[1:]], axis=1)
    band_docs = jnp.concatenate([key_docs[:-1], key_docs[1:]], axis=1)
    band_place = jnp.concatenate([key_place[:-1], key_place[1:]], axis=1)
    query_docs = documents.reshape(block_list, WINDOW_REACH)
    grouped_queries = queries.reshape(block_list, WINDOW_REACH, kv_heads, query_group, HEAD_SIZE)
    scores = jnp.einsum(
        "nqhgd,nshd->nhgqs", grouped_queries, band_keys, preferred_element_type=jnp.float32
    ) * HEAD_SIZE ** (-0.5)
    row_index = jnp.arange(WINDOW_REACH, dtype=jnp.int32)[:, None]
    col_index = jnp.arange(2 * WINDOW_REACH, dtype=jnp.int32)[None, :]
    distance = WINDOW_REACH + row_index - col_index
    near = (distance >= 0) & (distance < WINDOW_REACH)
    visible = (
        near[None]
        & (band_docs[:, None, :] == query_docs[:, :, None])
        & (band_place[:, None, :] >= 0)
    )
    visible = visible[:, None, None]
    head_sink_logit = sinks.reshape(kv_heads, query_group)[None, :, :, None]
    scores = jnp.where(visible, scores, masked_score)
    top = jnp.maximum(jnp.max(scores, axis=-1), head_sink_logit)
    exponent = jnp.where(visible, jnp.exp(scores - top[..., None]), 0.0)
    total = jnp.exp(head_sink_logit - top) + jnp.sum(exponent, axis=-1)
    shares = (exponent / total[..., None]).astype(jnp.bfloat16)
    attended = jnp.einsum(
        "nhgqs,nshd->nqhgd", shares, band_values, preferred_element_type=jnp.float32
    )
    return attended.astype(jnp.bfloat16).reshape(length, heads * HEAD_SIZE)


def rotated(shard, axis, by):
    peers = lax.axis_size(axis)
    return lax.ppermute(shard, axis, [(i, (i + by) % peers) for i in range(peers)])


def row_block(array, index, rows):
    return lax.dynamic_slice_in_dim(array, index * rows, rows, axis=0)


def gathered_body(
    queries, keys, values, documents, sinks, out_weight, residual, norm_gain, up_weight, down_weight
):
    up_whole, down_whole = (
        lax.all_gather(up_weight, "sp", axis=0, tiled=True),
        lax.all_gather(down_weight, "sp", axis=1, tiled=True),
    )
    n_tp = lax.axis_size("tp")
    me = lax.axis_index("tp")
    rows = residual.shape[0]
    attended = windowed_attention(queries, keys, values, documents, sinks)
    width = attended.shape[1]
    token_heads = jnp.zeros((rows, width * n_tp), jnp.bfloat16)
    for by in range(n_tp):
        piece = row_block(attended, (me + by) % n_tp, rows)
        if by:
            piece = rotated(piece, "tp", by)
        token_heads = lax.dynamic_update_slice_in_dim(
            token_heads, piece, ((me - by) % n_tp) * width, axis=1
        )
    projected = jnp.dot(token_heads, out_weight, preferred_element_type=jnp.float32)
    mixed = rounded(residual.astype(jnp.float32) + rounded(projected).astype(jnp.float32))
    widened = mixed.astype(jnp.float32)
    normed = (
        widened
        * lax.rsqrt(jnp.mean(widened * widened, axis=-1, keepdims=True) + epsilon)
        * norm_gain
    ).astype(jnp.bfloat16)
    branch = 0.0
    for by in range(n_tp - 1, -1, -1):
        rows_in = rotated(normed, "tp", by) if by else normed
        hidden = squared_relu(jnp.dot(rows_in, up_whole, preferred_element_type=jnp.float32))
        partial = jnp.dot(hidden, down_whole, preferred_element_type=jnp.float32).astype(
            jnp.bfloat16
        )
        if by:
            partial = rotated(partial, "tp", n_tp - by)
        branch = branch + partial.astype(jnp.float32)
    return (widened + rounded(branch).astype(jnp.float32)).astype(jnp.bfloat16)


def fits(mesh, tokens, width, kv_width, model, hidden):
    n_sp, n_tp = mesh.shape["sp"], mesh.shape["tp"]
    block = model // n_sp
    return (
        n_tp == 2
        and n_sp % (n_tp * CORES) == 0
        and n_sp // (n_tp * CORES) >= 3
        and block % LANES == 0
        and kv_width == LANES
        and width % (2 * LANES) == 0
        and tokens % (2 * WINDOW_REACH // 2) == 0
        and (tokens // n_tp) % 32 == 0
        and hidden % (n_tp * 2 * LANES) == 0
    )


def layer_kernel(
    n_z,
    q_hbm, k_hbm, v_hbm, docs_flat, sinks, outw_hbm, res_hbm, gain_ref, up_hbm, down_hbm,
    out_ref,
    up_all, down_all, rows_all, hid_all, outw, res, mixed, q_ref, k_ref, v_ref, docs, docs_prev,
    k_wide, v_wide, att, oth, psend, precv, own_sum,
    load_sem, halo_send, halo_recv, xs_sem, xr_sem, z_send, z_recv, d_send, d_recv, y_sem,
    g_send, g_recv, p_send, p_recv, own_sem,
):
    sp, y = lax.axis_index("sp"), lax.axis_index("tp")
    n_x, n_y = 2, 2
    z, x, c = sp // (n_x * CORES), lax.rem(sp // CORES, n_x), lax.rem(sp, CORES)
    n_sp = n_z * n_x * CORES
    tokens = q_ref.shape[0]
    rows = res.shape[0]
    half = rows // 2
    model = res.shape[1]
    width = q_ref.shape[1]
    blk = up_hbm.shape[0]
    quarter = up_hbm.shape[1] // n_x
    wide = 2 * blk

    def at(zz, xx, yy, cc):
        return ((zz * n_x + xx) * CORES + cc, yy)

    def remote(src, dst, send, recv, dev):
        return pltpu.make_async_remote_copy(
            src_ref=src, dst_ref=dst, send_sem=send, recv_sem=recv, device_id=dev, device_id_type=MESH
        )

    x_peer, y_peer, c_peer = at(z, 1 - x, y, c), at(z, x, 1 - y, c), at(z, x, y, 1 - c)

    def block(phase, zb, xb, cb):
        if phase == 0:
            first = ((zb * n_x + xb) * CORES + cb) * blk
            return up_all.at[pl.ds(pl.multiple_of(first, blk), blk), :]
        return down_all.at[zb * n_x + xb, :, pl.ds(pl.multiple_of(cb * blk, blk), blk)]

    def own_piece(phase, xq):
        start = pl.multiple_of(xq * quarter, quarter)
        if phase == 0:
            return up_hbm.at[:, pl.ds(start, quarter)]
        return down_hbm.at[pl.ds(start, quarter), :]

    def part_of(ref, h):
        size = ref.shape[0] // 2
        return ref.at[pl.ds(h * size, size), :]

    def x_exchange(phase, h):
        return remote(
            part_of(own_piece(phase, 1 - x), h), part_of(block(phase, z, x, c), h),
            xs_sem.at[phase, h], xr_sem.at[phase, h], x_peer,
        )

    def own_load(phase):
        return pltpu.make_async_copy(own_piece(phase, x), block(phase, z, x, c), own_sem.at[phase])

    low = jnp.minimum(z, n_z - 1 - z)
    inward = jnp.where(2 * z < n_z, 1, -1)

    def plane(k):
        near = z + jnp.where(lax.rem(k, 2) == 1, inward, -inward) * ((k + 1) // 2)
        far = jnp.where(z < n_z - 1 - z, k, n_z - 1 - k)
        return jnp.where(k <= 2 * low, near, far)

    def place(t):
        zb, b = plane(t // 2), lax.rem(t, 2)
        return zb, b, jnp.where(b == 0, x, 1 - x)

    def to_up(phase, zb, b, xb):
        ref = block(phase, zb, xb, c)
        return remote(ref, ref, z_send.at[0, phase, zb, b], z_recv.at[phase, zb, b], at(z + 1, x, y, c))

    def to_down(phase, zb, b, xb):
        ref = block(phase, zb, xb, c)
        return remote(ref, ref, z_send.at[1, phase, zb, b], z_recv.at[phase, zb, b], at(z - 1, x, y, c))

    def to_core(phase, zb, b, xb):
        ref = block(phase, zb, xb, c)
        return remote(ref, ref, d_send.at[phase, zb, b], d_recv.at[phase, zb, b], c_peer)

    def goes_up(zb):
        return jnp.logical_and(zb <= z, z < n_z - 1)

    def goes_down(zb):
        return jnp.logical_and(zb >= z, z > 0)

    def pass_on(phase, t):
        zb, b, xb = place(t)

        @pl.when(goes_up(zb))
        def _():
            to_up(phase, zb, b, xb).start()

        @pl.when(goes_down(zb))
        def _():
            to_down(phase, zb, b, xb).start()

        to_core(phase, zb, b, xb).start()

    def arrive_x(phase, h):
        x_exchange(phase, h).wait_recv()
        ref = part_of(block(phase, z, 1 - x, c), h)

        @pl.when(z < n_z - 1)
        def _():
            remote(
                ref, ref, z_send.at[0, phase, z, 1], z_recv.at[phase, z, 1], at(z + 1, x, y, c)
            ).start()

        @pl.when(z > 0)
        def _():
            remote(
                ref, ref, z_send.at[1, phase, z, 1], z_recv.at[phase, z, 1], at(z - 1, x, y, c)
            ).start()

        if h == 1:
            to_core(phase, z, 1, 1 - x).start()

    def arrive(phase, t):
        zb, b, xb = place(t)
        to_up(phase, zb, b, xb).wait_recv()
        pass_on(phase, t)

    last = tokens - WINDOW_REACH
    nxt = (sp + 1, y)

    def halo(i):
        src, dst = (
            (k_hbm.at[pl.ds(last, WINDOW_REACH), :], k_ref.at[pl.ds(0, WINDOW_REACH), :]),
            (v_hbm.at[pl.ds(last, WINDOW_REACH), :], v_ref.at[pl.ds(0, WINDOW_REACH), :]),
            (docs_flat, docs_prev),
        )[i]
        return remote(src, dst, halo_send.at[i], halo_recv.at[i], nxt)

    own_load(0).start()
    barrier = pltpu.get_barrier_semaphore()
    partners = (
        (True, x_peer), (True, y_peer), (True, at(z, 1 - x, 1 - y, c)), (True, c_peer),
        (z < n_z - 1, at(z + 1, x, y, c)), (z > 0, at(z - 1, x, y, c)),
        (sp < n_sp - 1, nxt), (sp > 0, (sp - 1, y)),
    )
    for here, dev in partners:
        @pl.when(here)
        def _():
            pl.semaphore_signal(barrier, inc=1, device_id=dev, device_id_type=MESH)

    pl.semaphore_wait(barrier, sum(jnp.int32(here) for here, _ in partners))

    @pl.when(sp < n_sp - 1)
    def _():
        for i in range(3):
            halo(i).start()

    loads = [
        pltpu.make_async_copy(q_hbm, q_ref, load_sem.at[0]),
        pltpu.make_async_copy(k_hbm, k_ref.at[pl.ds(WINDOW_REACH, tokens), :], load_sem.at[1]),
        pltpu.make_async_copy(v_hbm, v_ref.at[pl.ds(WINDOW_REACH, tokens), :], load_sem.at[2]),
        pltpu.make_async_copy(outw_hbm, outw, load_sem.at[3]),
        pltpu.make_async_copy(res_hbm, res, load_sem.at[4]),
    ]
    own_load(0).wait()

    def begin():
        x_exchange(0, 0).start()
        pass_on(0, 0)
        x_exchange(0, 1).start()

    @pl.when(c == 1)
    def _():
        begin()

    for load in loads:
        load.start()
    own_load(1).start()

    @pl.when(sp == 0)
    def _():
        k_ref[pl.ds(0, WINDOW_REACH), :] = jnp.zeros((WINDOW_REACH, LANES), jnp.bfloat16)
        v_ref[pl.ds(0, WINDOW_REACH), :] = jnp.zeros((WINDOW_REACH, LANES), jnp.bfloat16)
        docs_prev[...] = jnp.full(docs_prev.shape, -1, jnp.int32)

    for load in loads[:3]:
        load.wait()

    @pl.when(sp > 0)
    def _():
        for i in range(3):
            halo(i).wait_recv()

    docs[0, 0] = docs_prev[last:]
    for i in range(tokens // LANES):
        docs[i + 1, 0] = docs_flat[i * LANES : (i + 1) * LANES]
    @pl.when(c == 0)
    def _():
        begin()

    heads = width // HEAD_SIZE
    kv_heads = LANES // HEAD_SIZE
    group = heads // kv_heads
    lane_in = lax.broadcasted_iota(jnp.int32, (LANES, LANES), 0)
    lane_out = lax.broadcasted_iota(jnp.int32, (LANES, LANES), 1)
    for g in range(kv_heads):
        for par in range(2):
            pick = (lane_in - g * HEAD_SIZE == lane_out - par * HEAD_SIZE) & (
                lane_out // HEAD_SIZE == par
            )
            pick = pick.astype(jnp.float32).astype(jnp.bfloat16)
            for raw, spread in ((k_ref, k_wide), (v_ref, v_wide)):
                spread[g * 2 + par] = jnp.dot(
                    raw[...], pick, preferred_element_type=jnp.float32
                ).astype(jnp.bfloat16)

    row_i = lax.broadcasted_iota(jnp.int32, (WINDOW_REACH, 2 * WINDOW_REACH), 0)
    col_i = lax.broadcasted_iota(jnp.int32, (WINDOW_REACH, 2 * WINDOW_REACH), 1)
    near = (col_i > row_i) & (col_i <= row_i + WINDOW_REACH)

    def attend(n, carry):
        start = pl.multiple_of(n * WINDOW_REACH, WINDOW_REACH)
        early = jnp.broadcast_to(docs[n], (WINDOW_REACH, LANES))
        late = jnp.broadcast_to(docs[n + 1], (WINDOW_REACH, LANES))
        mine = late.T
        same = jnp.concatenate([early == mine, late == mine], axis=1)
        visible = near & same
        for j in range(width // LANES):
            total_out = None
            g = (2 * j) // group
            q_blk = q_ref[pl.ds(start, WINDOW_REACH), j * LANES : (j + 1) * LANES]
            for par in range(2):
                head = 2 * j + par
                keys = k_wide[g * 2 + par, pl.ds(start, 2 * WINDOW_REACH), :]
                vals = v_wide[g * 2 + par, pl.ds(start, 2 * WINDOW_REACH), :]
                scores = lax.dot_general(
                    q_blk, keys, (((1,), (1,)), ((), ())), preferred_element_type=jnp.float32
                ) * HEAD_SIZE ** (-0.5)
                scores = jnp.where(visible, scores, masked_score)
                sink = sinks[head]
                top = jnp.maximum(jnp.max(scores, axis=1, keepdims=True), sink)
                exponent = jnp.where(visible, jnp.exp(scores - top), 0.0)
                total = jnp.exp(sink - top) + jnp.sum(exponent, axis=1, keepdims=True)
                shares = (exponent * (1.0 / total)).astype(jnp.bfloat16)
                part = jnp.dot(shares, vals, preferred_element_type=jnp.float32)
                total_out = part if total_out is None else total_out + part
            att[pl.ds(start, WINDOW_REACH), j * LANES : (j + 1) * LANES] = total_out.astype(
                jnp.bfloat16
            )

        @pl.when(n == steps // 2 + 1)
        def _():
            arrive_x(0, 0)

        return carry

    steps = tokens // WINDOW_REACH
    lax.fori_loop(0, steps, attend, 0)

    mine_at = pl.multiple_of(y * rows, rows)
    theirs_at = pl.multiple_of((1 - y) * rows, rows)
    swap = remote(att.at[pl.ds(theirs_at, rows), :], oth, y_sem.at[0], y_sem.at[1], y_peer)
    swap.start()
    for h in range(2):
        x_exchange(1, h).start()
    arrive_x(0, 1)
    arrive(0, 2)
    loads[3].wait()
    loads[4].wait()
    swap.wait_recv()

    me_p = x * n_y + y
    x_p, y_p, d_p = (1 - x) * n_y + y, x * n_y + 1 - y, (1 - x) * n_y + 1 - y
    chunk = 2 * wide

    def row_part(p, h):
        return rows_all.at[pl.ds(pl.multiple_of(p * rows + h * half, half), half), :]

    def give(p, h, way):
        slot = p * 2 + h
        ref = row_part(p, h)
        return remote(ref, ref, g_send.at[way, slot], g_recv.at[slot], x_peer if way == 0 else y_peer)

    for h in range(2):
        own_rows = pl.ds(pl.multiple_of(mine_at + h * half, half), half)

        def project(n, square):
            cols = pl.ds(pl.multiple_of(n * chunk, chunk), chunk)
            acc = jnp.dot(
                att[own_rows, :], outw[pl.ds(pl.multiple_of(y * width, width), width), cols],
                preferred_element_type=jnp.float32,
            ) + jnp.dot(
                oth[h * half : (h + 1) * half, :],
                outw[pl.ds(pl.multiple_of((1 - y) * width, width), width), cols],
                preferred_element_type=jnp.float32,
            )
            sums = res[h * half : (h + 1) * half, cols].astype(jnp.float32) + acc.astype(
                jnp.bfloat16
            ).astype(jnp.float32)
            sums = sums.astype(jnp.bfloat16)
            mixed[h * half : (h + 1) * half, cols] = sums
            sums = sums.astype(jnp.float32)
            return square + jnp.sum(sums * sums, axis=1, keepdims=True)

        square = lax.fori_loop(0, model // chunk, project, jnp.zeros((half, 1), jnp.float32))
        scale = lax.rsqrt(square * (1.0 / model) + epsilon)

        def normalise(n, carry):
            cols = pl.ds(pl.multiple_of(n * chunk, chunk), chunk)
            wide_rows = mixed[h * half : (h + 1) * half, cols].astype(jnp.float32)
            rows_all[pl.ds(pl.multiple_of(me_p * rows + h * half, half), half), cols] = (
                wide_rows * scale * gain_ref[:, cols]
            ).astype(jnp.bfloat16)
            return carry

        lax.fori_loop(0, model // chunk, normalise, 0)
        give(me_p, h, 0).start()
        give(me_p, h, 1).start()

    arrive(0, 3)
    n_items = 2 * n_z

    def more(first, until):
        for t in range(first, min(until, n_items)):
            arrive(0, t)

    more(4, 6)
    give(x_p, 0, 0).wait_recv()
    give(x_p, 0, 1).start()
    more(6, 7)
    give(y_p, 1, 1).wait_recv()
    give(y_p, 1, 0).start()
    more(7, n_items)

    own_load(1).wait()
    pass_on(1, 0)
    for h in range(2):
        arrive_x(1, h)

    give(x_p, 1, 0).wait_recv()
    give(y_p, 0, 1).wait_recv()
    give(d_p, 0, 1).wait_recv()
    give(d_p, 1, 0).wait_recv()

    def core_wait(phase):
        def wait_one(t, carry):
            zb, b, xb = place(t)
            to_core(phase, zb, b, xb).wait_recv()
            return carry
        return wait_one

    lax.fori_loop(0, n_items, core_wait(0), 0)
    tall = 2 * rows

    def up_step(i, carry):
        r = pl.ds(pl.multiple_of((i // (quarter // chunk)) * tall, tall), tall)
        f = pl.ds(pl.multiple_of(lax.rem(i, quarter // chunk) * chunk, chunk), chunk)
        before = jnp.dot(rows_all[r, :], up_all[:, f], preferred_element_type=jnp.float32)
        before = jnp.maximum(before, 0.0)
        hid_all[r, f] = (before * before).astype(jnp.bfloat16)
        return carry

    lax.fori_loop(0, 2 * (quarter // chunk), up_step, 0)

    def lanes(ref, h):
        return ref if h is None else ref.at[:, pl.ds(h * blk, blk)]

    def way(s):
        return jnp.where(s >= 2, 1 - x, x), jnp.where(lax.rem(s, 2) == 1, 1 - y, y)

    def partial_copy(j, s, h=None):
        px, py = way(s)
        return remote(
            lanes(psend.at[j, s - 1], h), lanes(precv.at[j, s - 1], h),
            p_send.at[j, h or 0, s - 1], p_recv.at[j, h or 0, s - 1], at(z, px, py, c),
        )

    def pair_of(t):
        zb, b, xb = place(t)
        return zb * n_x + xb

    def combine(t, h=None):
        j = pair_of(t)
        total = lanes(own_sum.at[j], h)[...]
        for s in (1, 2, 3):
            partial_copy(j, s, h).wait_recv()
            total = total + lanes(precv.at[j, s - 1], h)[...].astype(jnp.float32)
        size = wide if h is None else blk
        cols = pl.ds(pl.multiple_of(j * wide + (h or 0) * blk, blk), size)
        out_ref[:, cols] = (
            mixed[:, cols].astype(jnp.float32) + total.astype(jnp.bfloat16).astype(jnp.float32)
        ).astype(jnp.bfloat16)

    def pieces(j, h=None):
        def piece(i, carry):
            s = 3 - i
            px, py = way(s)
            first = pl.multiple_of((px * n_y + py) * rows, rows)
            part = jnp.dot(
                hid_all[pl.ds(first, rows), :], lanes(down_all.at[j], h)[...],
                preferred_element_type=jnp.float32,
            )

            @pl.when(s > 0)
            def _():
                lanes(psend.at[j, s - 1], h)[...] = part.astype(jnp.bfloat16)
                partial_copy(j, s, h).start()

            @pl.when(s == 0)
            def _():
                lanes(own_sum.at[j], h)[...] = part

            return carry

        lax.fori_loop(0, n_x * n_y, piece, 0)

    lag = 4
    n_whole = n_items - 2

    def blocks_sent(phase, t):
        zb, b, xb = place(t)

        @pl.when(goes_up(zb))
        def _():
            to_up(phase, zb, b, xb).wait_send()

        @pl.when(goes_down(zb))
        def _():
            to_down(phase, zb, b, xb).wait_send()

        to_core(phase, zb, b, xb).wait_send()

    def partials_sent(t, carry):
        j = pair_of(t)
        for s in (1, 2, 3):
            @pl.when(t < n_whole)
            def _():
                partial_copy(j, s).wait_send()

            @pl.when(t >= n_whole)
            def _():
                for h in range(2):
                    partial_copy(j, s, h).wait_send()

        return carry

    @pl.when(sp < n_sp - 1)
    def _():
        for i in range(3):
            halo(i).wait_send()

    swap.wait_send()
    for phase in range(2):
        for h in range(2):
            x_exchange(phase, h).wait_send()

    def down_step(t, carry):
        @pl.when(t >= 2)
        def _():
            arrive(1, t)

        zb, b, xb = place(t)
        to_core(1, zb, b, xb).wait_recv()
        pieces(pair_of(t))

        @pl.when(t >= lag)
        def _():
            combine(t - lag)
            partials_sent(t - lag, 0)

        blocks_sent(0, t)
        return carry

    lax.fori_loop(0, n_whole, down_step, 0)

    def last_step(t, carry):
        for h in (1, 0):
            @pl.when(c == h)
            def _():
                arrive(1, t)

            @pl.when(c != h)
            def _():
                zb, b, xb = place(t)
                to_core(1, zb, b, xb).wait_recv()

            pieces(pair_of(t), h)
            done = n_whole - lag + 2 * (t - n_whole) + 1 - h

            @pl.when(done < n_whole - 1)
            def _():
                combine(done)
                partials_sent(done, 0)

        blocks_sent(0, t)
        return carry

    lax.fori_loop(n_whole, n_items, last_step, 0)
    for h in range(2):
        give(me_p, h, 0).wait_send()
        give(me_p, h, 1).wait_send()
    give(x_p, 0, 1).wait_send()
    give(y_p, 1, 0).wait_send()

    def down_sent(t, carry):
        blocks_sent(1, t)
        return carry

    lax.fori_loop(0, n_items, down_sent, 0)
    for t in range(n_whole - 1, n_items):
        for h in (None,) if t < n_whole else (1, 0):
            combine(jnp.int32(t), h)

    lax.fori_loop(n_whole - 1, n_items, partials_sent, 0)


def kernel_body(
    n_z, queries, keys, values, documents, sinks, out_weight, residual, norm_gain, up_weight, down_weight
):
    tokens, width = queries.shape
    rows, model = residual.shape
    blk, hidden = up_weight.shape
    quarter = hidden // 2
    group = 4 * rows
    pairs = 2 * n_z
    bf16, f32 = jnp.bfloat16, jnp.float32
    hbm = pl.BlockSpec(memory_space=pl.ANY)
    dma = pltpu.SemaphoreType.DMA
    return pl.pallas_call(
        functools.partial(layer_kernel, n_z),
        out_shape=pltpu.VMEM((rows, model), bf16),
        in_specs=[hbm, hbm, hbm, pl.BlockSpec(memory_space=pltpu.VMEM), pl.BlockSpec(memory_space=pltpu.SMEM), hbm, hbm,
                  pl.BlockSpec(memory_space=pltpu.VMEM), hbm, hbm],
        out_specs=pl.BlockSpec(memory_space=pltpu.VMEM),
        scratch_shapes=[
            pltpu.VMEM((model, quarter), bf16),
            pltpu.VMEM((pairs, quarter, 2 * blk), bf16),
            pltpu.VMEM((group, model), bf16),
            pltpu.VMEM((group, quarter), bf16),
            pltpu.VMEM(out_weight.shape, bf16),
            pltpu.VMEM((rows, model), bf16),
            pltpu.VMEM((rows, model), bf16),
            pltpu.VMEM((tokens, width), bf16),
            pltpu.VMEM((tokens + WINDOW_REACH, LANES), bf16),
            pltpu.VMEM((tokens + WINDOW_REACH, LANES), bf16),
            pltpu.VMEM((tokens // LANES + 1, 1, LANES), jnp.int32),
            pltpu.VMEM((tokens,), jnp.int32),
            pltpu.VMEM((4, tokens + WINDOW_REACH, LANES), bf16),
            pltpu.VMEM((4, tokens + WINDOW_REACH, LANES), bf16),
            pltpu.VMEM((tokens, width), bf16),
            pltpu.VMEM((rows, width), bf16),
            pltpu.VMEM((pairs, 3, rows, 2 * blk), bf16),
            pltpu.VMEM((pairs, 3, rows, 2 * blk), bf16),
            pltpu.VMEM((pairs, rows, 2 * blk), f32),
            dma((6,)), dma((3,)), dma((3,)), dma((2, 2)), dma((2, 2)), dma((2, 2, n_z, 2)), dma((2, n_z, 2)),
            dma((2, n_z, 2)), dma((2, n_z, 2)), dma((2,)), dma((2, 8)), dma((8,)),
            dma((pairs, 2, 3)), dma((pairs, 2, 3)), dma((2,)),
        ],
        compiler_params=pltpu.CompilerParams(collective_id=0, has_side_effects=True, vmem_limit_bytes=60 << 20),
    )(
        queries, keys, values, documents, sinks, out_weight,
        residual, norm_gain.reshape(1, model), up_weight, down_weight,
    )


def body(n_z, mesh, *arrays):
    queries, keys, up_weight, residual = arrays[0], arrays[1], arrays[8], arrays[6]
    if fits(mesh, *queries.shape, keys.shape[1], residual.shape[1], up_weight.shape[1]):
        return kernel_body(n_z, *arrays)
    return gathered_body(*arrays)


def solution(mesh):
    in_specs = (
        P("sp", "tp"),
        P("sp", "tp"),
        P("sp", "tp"),
        P("sp"),
        P("tp"),
        P(),
        P(("sp", "tp"), None),
        P(),
        P("sp", "tp"),
        P("tp", "sp"),
    )
    out_specs = P(("sp", "tp"), None)
    n_z = mesh.shape["sp"] // (CORES * mesh.shape["tp"])
    return jax.shard_map(
        functools.partial(body, n_z, mesh), mesh=mesh, in_specs=in_specs, out_specs=out_specs, check_vma=False
    )
```

```python
import functools

import jax
import jax.numpy as jnp
from jax import lax
from jax.experimental import pallas as pl
from jax.experimental.pallas import tpu as pltpu
from jax.sharding import PartitionSpec as P

HEAD_SIZE = 64
WINDOW_REACH = 128
LANES = 128
CORES = 2
MESH = pl.DeviceIdType.MESH

masked_score = -1e30
epsilon = 1e-06


def passed_along(shard, axis, by):
    peers = lax.axis_size(axis)
    pairs = [(i, i + by) for i in range(peers) if 0 <= i + by < peers]
    return lax.ppermute(shard, axis, pairs)


def rounded(value):
    return lax.optimization_barrier(value.astype(jnp.bfloat16))


def squared_relu(before):
    return jnp.square(jax.nn.relu(before)).astype(jnp.bfloat16)


def windowed_attention(queries, keys, values, documents, sinks):
    length = queries.shape[0]
    heads = queries.shape[1] // HEAD_SIZE
    kv_heads = keys.shape[1] // HEAD_SIZE
    query_group = heads // kv_heads
    block_list = length // WINDOW_REACH
    prev_keys, prev_values, prev_docs = passed_along(
        (
            keys[length - WINDOW_REACH :],
            values[length - WINDOW_REACH :],
            documents[length - WINDOW_REACH :],
        ),
        "sp",
        1,
    )
    offset = lax.axis_index("sp") * length
    key_matrix = jnp.concatenate([prev_keys, keys], axis=0).reshape(
        block_list + 1, WINDOW_REACH, kv_heads, HEAD_SIZE
    )
    value_matrix = jnp.concatenate([prev_values, values], axis=0).reshape(
        block_list + 1, WINDOW_REACH, kv_heads, HEAD_SIZE
    )
    key_docs = jnp.concatenate([prev_docs, documents], axis=0).reshape(block_list + 1, WINDOW_REACH)
    key_place = (
        offset - WINDOW_REACH + jnp.arange((block_list + 1) * WINDOW_REACH, dtype=jnp.int32)
    ).reshape(block_list + 1, WINDOW_REACH)
    band_keys = jnp.concatenate([key_matrix[:-1], key_matrix[1:]], axis=1)
    band_values = jnp.concatenate([value_matrix[:-1], value_matrix[1:]], axis=1)
    band_docs = jnp.concatenate([key_docs[:-1], key_docs[1:]], axis=1)
    band_place = jnp.concatenate([key_place[:-1], key_place[1:]], axis=1)
    query_docs = documents.reshape(block_list, WINDOW_REACH)
    grouped_queries = queries.reshape(block_list, WINDOW_REACH, kv_heads, query_group, HEAD_SIZE)
    scores = jnp.einsum(
        "nqhgd,nshd->nhgqs", grouped_queries, band_keys, preferred_element_type=jnp.float32
    ) * HEAD_SIZE ** (-0.5)
    row_index = jnp.arange(WINDOW_REACH, dtype=jnp.int32)[:, None]
    col_index = jnp.arange(2 * WINDOW_REACH, dtype=jnp.int32)[None, :]
    distance = WINDOW_REACH + row_index - col_index
    near = (distance >= 0) & (distance < WINDOW_REACH)
    visible = (
        near[None]
        & (band_docs[:, None, :] == query_docs[:, :, None])
        & (band_place[:, None, :] >= 0)
    )
    visible = visible[:, None, None]
    head_sink_logit = sinks.reshape(kv_heads, query_group)[None, :, :, None]
    scores = jnp.where(visible, scores, masked_score)
    top = jnp.maximum(jnp.max(scores, axis=-1), head_sink_logit)
    exponent = jnp.where(visible, jnp.exp(scores - top[..., None]), 0.0)
    total = jnp.exp(head_sink_logit - top) + jnp.sum(exponent, axis=-1)
    shares = (exponent / total[..., None]).astype(jnp.bfloat16)
    attended = jnp.einsum(
        "nhgqs,nshd->nqhgd", shares, band_values, preferred_element_type=jnp.float32
    )
    return attended.astype(jnp.bfloat16).reshape(length, heads * HEAD_SIZE)


def rotated(shard, axis, by):
    peers = lax.axis_size(axis)
    return lax.ppermute(shard, axis, [(i, (i + by) % peers) for i in range(peers)])


def row_block(array, index, rows):
    return lax.dynamic_slice_in_dim(array, index * rows, rows, axis=0)


def gathered_body(
    queries, keys, values, documents, sinks, out_weight, residual, norm_gain, up_weight, down_weight
):
    up_whole, down_whole = (
        lax.all_gather(up_weight, "sp", axis=0, tiled=True),
        lax.all_gather(down_weight, "sp", axis=1, tiled=True),
    )
    n_tp = lax.axis_size("tp")
    me = lax.axis_index("tp")
    rows = residual.shape[0]
    attended = windowed_attention(queries, keys, values, documents, sinks)
    width = attended.shape[1]
    token_heads = jnp.zeros((rows, width * n_tp), jnp.bfloat16)
    for by in range(n_tp):
        piece = row_block(attended, (me + by) % n_tp, rows)
        if by:
            piece = rotated(piece, "tp", by)
        token_heads = lax.dynamic_update_slice_in_dim(
            token_heads, piece, ((me - by) % n_tp) * width, axis=1
        )
    projected = jnp.dot(token_heads, out_weight, preferred_element_type=jnp.float32)
    mixed = rounded(residual.astype(jnp.float32) + rounded(projected).astype(jnp.float32))
    widened = mixed.astype(jnp.float32)
    normed = (
        widened
        * lax.rsqrt(jnp.mean(widened * widened, axis=-1, keepdims=True) + epsilon)
        * norm_gain
    ).astype(jnp.bfloat16)
    branch = 0.0
    for by in range(n_tp - 1, -1, -1):
        rows_in = rotated(normed, "tp", by) if by else normed
        hidden = squared_relu(jnp.dot(rows_in, up_whole, preferred_element_type=jnp.float32))
        partial = jnp.dot(hidden, down_whole, preferred_element_type=jnp.float32).astype(
            jnp.bfloat16
        )
        if by:
            partial = rotated(partial, "tp", n_tp - by)
        branch = branch + partial.astype(jnp.float32)
    return (widened + rounded(branch).astype(jnp.float32)).astype(jnp.bfloat16)


def fits(mesh, tokens, width, kv_width, model, hidden):
    n_sp, n_tp = mesh.shape["sp"], mesh.shape["tp"]
    block = model // n_sp
    return (
        n_tp == 2
        and n_sp % (n_tp * CORES) == 0
        and n_sp // (n_tp * CORES) >= 3
        and block % LANES == 0
        and kv_width == LANES
        and width % (2 * LANES) == 0
        and tokens % (2 * WINDOW_REACH // 2) == 0
        and (tokens // n_tp) % 32 == 0
        and hidden % (n_tp * 2 * LANES) == 0
    )


def layer_kernel(
    n_z,
    q_hbm, k_hbm, v_hbm, docs_hbm, sinks_hbm, outw_hbm, res_hbm, gain_hbm, up_hbm, down_hbm,
    out_ref,
    up_all, down_all, rows_all, hid_all, outw, res, mixed, q_ref, k_ref, v_ref, docs, docs_prev, docs_flat, sinks, gain_ref,
    k_wide, v_wide, att, oth, psend, precv, own_sum,
    load_sem, halo_send, halo_recv, xs_sem, xr_sem, z_send, z_recv, d_send, d_recv, y_sem,
    g_send, g_recv, p_send, p_recv, own_sem,
):
    sp, y = lax.axis_index("sp"), lax.axis_index("tp")
    n_x, n_y = 2, 2
    z, x, c = sp // (n_x * CORES), lax.rem(sp // CORES, n_x), lax.rem(sp, CORES)
    n_sp = n_z * n_x * CORES
    tokens = q_ref.shape[0]
    rows = res.shape[0]
    half = rows // 2
    model = res.shape[1]
    width = q_ref.shape[1]
    blk = up_hbm.shape[0]
    quarter = up_hbm.shape[1] // n_x
    wide = 2 * blk

    def at(zz, xx, yy, cc):
        return ((zz * n_x + xx) * CORES + cc, yy)

    def remote(src, dst, send, recv, dev):
        return pltpu.make_async_remote_copy(
            src_ref=src, dst_ref=dst, send_sem=send, recv_sem=recv, device_id=dev, device_id_type=MESH
        )

    x_peer, y_peer, c_peer = at(z, 1 - x, y, c), at(z, x, 1 - y, c), at(z, x, y, 1 - c)

    def block(phase, zb, xb, cb):
        if phase == 0:
            first = ((zb * n_x + xb) * CORES + cb) * blk
            return up_all.at[pl.ds(pl.multiple_of(first, blk), blk), :]
        return down_all.at[zb * n_x + xb, :, pl.ds(pl.multiple_of(cb * blk, blk), blk)]

    def own_piece(phase, xq):
        start = pl.multiple_of(xq * quarter, quarter)
        if phase == 0:
            return up_hbm.at[:, pl.ds(start, quarter)]
        return down_hbm.at[pl.ds(start, quarter), :]

    def part_of(ref, h):
        size = ref.shape[0] // 2
        return ref.at[pl.ds(h * size, size), :]

    def x_exchange(phase, h):
        return remote(
            part_of(own_piece(phase, 1 - x), h), part_of(block(phase, z, x, c), h),
            xs_sem.at[phase], xr_sem.at[phase, h], x_peer,
        )

    def own_load(phase):
        return pltpu.make_async_copy(own_piece(phase, x), block(phase, z, x, c), own_sem.at[phase])

    low = jnp.minimum(z, n_z - 1 - z)
    inward = jnp.where(2 * z < n_z, 1, -1)

    def plane(k):
        near = z + jnp.where(lax.rem(k, 2) == 1, inward, -inward) * ((k + 1) // 2)
        far = jnp.where(z < n_z - 1 - z, k, n_z - 1 - k)
        return jnp.where(k <= 2 * low, near, far)

    def place(t):
        zb, b = plane(t // 2), lax.rem(t, 2)
        return zb, b, jnp.where(b == 0, x, 1 - x)

    def to_up(phase, zb, b, xb):
        ref = block(phase, zb, xb, c)
        return remote(ref, ref, z_send.at[phase], z_recv.at[phase, zb, b], at(z + 1, x, y, c))

    def to_down(phase, zb, b, xb):
        ref = block(phase, zb, xb, c)
        return remote(ref, ref, z_send.at[phase], z_recv.at[phase, zb, b], at(z - 1, x, y, c))

    def to_core(phase, zb, b, xb):
        ref = block(phase, zb, xb, c)
        slot = 0 if phase == 0 else 1 + zb * n_x + b
        return remote(ref, ref, d_send.at[phase], d_recv.at[slot], c_peer)

    def to_core_all(phase):
        ref = up_all.at[pl.ds(0, model // 2), :] if phase == 0 else down_all.at[pl.ds(0, n_z)]
        return remote(ref, ref, d_send.at[phase], d_recv.at[0], c_peer)

    def goes_up(zb):
        return jnp.logical_and(zb <= z, z < n_z - 1)

    def goes_down(zb):
        return jnp.logical_and(zb >= z, z > 0)

    def pass_on(phase, t):
        zb, b, xb = place(t)

        @pl.when(goes_up(zb))
        def _():
            to_up(phase, zb, b, xb).start()

        @pl.when(goes_down(zb))
        def _():
            to_down(phase, zb, b, xb).start()

        to_core(phase, zb, b, xb).start()

    def arrive_x(phase, h):
        x_exchange(phase, h).wait_recv()
        ref = part_of(block(phase, z, 1 - x, c), h)

        @pl.when(z < n_z - 1)
        def _():
            remote(
                ref, ref, z_send.at[phase], z_recv.at[phase, z, 1], at(z + 1, x, y, c)
            ).start()

        @pl.when(z > 0)
        def _():
            remote(
                ref, ref, z_send.at[phase], z_recv.at[phase, z, 1], at(z - 1, x, y, c)
            ).start()

        if h == 1:
            to_core(phase, z, 1, 1 - x).start()

    def arrive(phase, t):
        zb, b, xb = place(t)
        to_up(phase, zb, b, xb).wait_recv()
        pass_on(phase, t)

    last = tokens - WINDOW_REACH
    nxt = (sp + 1, y)

    def halo(i):
        src, dst = (
            (k_hbm.at[pl.ds(last, WINDOW_REACH), :], k_ref.at[pl.ds(0, WINDOW_REACH), :]),
            (v_hbm.at[pl.ds(last, WINDOW_REACH), :], v_ref.at[pl.ds(0, WINDOW_REACH), :]),
            (docs_hbm, docs_prev),
        )[i]
        return remote(src, dst, halo_send.at[i], halo_recv.at[i], nxt)

    own_load(0).start()
    barrier = pltpu.get_barrier_semaphore()
    partners = (
        (True, x_peer), (True, y_peer), (True, at(z, 1 - x, 1 - y, c)), (True, c_peer),
        (z < n_z - 1, at(z + 1, x, y, c)), (z > 0, at(z - 1, x, y, c)),
        (sp < n_sp - 1, nxt), (sp > 0, (sp - 1, y)),
    )
    for here, dev in partners:
        @pl.when(here)
        def _():
            pl.semaphore_signal(barrier, inc=1, device_id=dev, device_id_type=MESH)

    pl.semaphore_wait(barrier, sum(jnp.int32(here) for here, _ in partners))

    @pl.when(sp < n_sp - 1)
    def _():
        for i in range(3):
            halo(i).start()

    loads = [
        pltpu.make_async_copy(q_hbm, q_ref, load_sem.at[0]),
        pltpu.make_async_copy(k_hbm, k_ref.at[pl.ds(WINDOW_REACH, tokens), :], load_sem.at[1]),
        pltpu.make_async_copy(v_hbm, v_ref.at[pl.ds(WINDOW_REACH, tokens), :], load_sem.at[2]),
        pltpu.make_async_copy(outw_hbm, outw, load_sem.at[3]),
        pltpu.make_async_copy(res_hbm, res, load_sem.at[4]),
        pltpu.make_async_copy(gain_hbm, gain_ref, load_sem.at[5]),
        pltpu.make_async_copy(docs_hbm, docs_flat, load_sem.at[6]),
        pltpu.make_async_copy(sinks_hbm, sinks, load_sem.at[7]),
    ]
    own_load(0).wait()

    def begin():
        x_exchange(0, 0).start()
        pass_on(0, 0)
        x_exchange(0, 1).start()

    @pl.when(c == 1)
    def _():
        begin()

    for load in loads:
        load.start()
    own_load(1).start()

    @pl.when(sp == 0)
    def _():
        k_ref[pl.ds(0, WINDOW_REACH), :] = jnp.zeros((WINDOW_REACH, LANES), jnp.bfloat16)
        v_ref[pl.ds(0, WINDOW_REACH), :] = jnp.zeros((WINDOW_REACH, LANES), jnp.bfloat16)
        docs_prev[...] = jnp.full(docs_prev.shape, -1, jnp.int32)

    for load in loads[:3] + loads[6:]:
        load.wait()

    @pl.when(sp > 0)
    def _():
        for i in range(3):
            halo(i).wait_recv()

    docs[0, 0] = docs_prev[last:]
    for i in range(tokens // LANES):
        docs[i + 1, 0] = docs_flat[i * LANES : (i + 1) * LANES]
    @pl.when(c == 0)
    def _():
        begin()

    heads = width // HEAD_SIZE
    kv_heads = LANES // HEAD_SIZE
    group = heads // kv_heads
    lane_in = lax.broadcasted_iota(jnp.int32, (LANES, LANES), 0)
    lane_out = lax.broadcasted_iota(jnp.int32, (LANES, LANES), 1)
    for g in range(kv_heads):
        for par in range(2):
            pick = (lane_in - g * HEAD_SIZE == lane_out - par * HEAD_SIZE) & (
                lane_out // HEAD_SIZE == par
            )
            pick = pick.astype(jnp.float32).astype(jnp.bfloat16)
            for raw, spread in ((k_ref, k_wide), (v_ref, v_wide)):
                spread[g * 2 + par] = jnp.dot(
                    raw[...], pick, preferred_element_type=jnp.float32
                ).astype(jnp.bfloat16)

    row_i = lax.broadcasted_iota(jnp.int32, (WINDOW_REACH, 2 * WINDOW_REACH), 0)
    col_i = lax.broadcasted_iota(jnp.int32, (WINDOW_REACH, 2 * WINDOW_REACH), 1)
    near = (col_i > row_i) & (col_i <= row_i + WINDOW_REACH)

    def attend(n, carry):
        start = pl.multiple_of(n * WINDOW_REACH, WINDOW_REACH)
        early = jnp.broadcast_to(docs[n], (WINDOW_REACH, LANES))
        late = jnp.broadcast_to(docs[n + 1], (WINDOW_REACH, LANES))
        mine = late.T
        same = jnp.concatenate([early == mine, late == mine], axis=1)
        visible = near & same
        for j in range(width // LANES):
            total_out = None
            g = (2 * j) // group
            q_blk = q_ref[pl.ds(start, WINDOW_REACH), j * LANES : (j + 1) * LANES]
            for par in range(2):
                head = 2 * j + par
                keys = k_wide[g * 2 + par, pl.ds(start, 2 * WINDOW_REACH), :]
                vals = v_wide[g * 2 + par, pl.ds(start, 2 * WINDOW_REACH), :]
                scores = lax.dot_general(
                    q_blk, keys, (((1,), (1,)), ((), ())), preferred_element_type=jnp.float32
                ) * HEAD_SIZE ** (-0.5)
                scores = jnp.where(visible, scores, masked_score)
                sink = sinks[head]
                top = jnp.maximum(jnp.max(scores, axis=1, keepdims=True), sink)
                exponent = jnp.where(visible, jnp.exp(scores - top), 0.0)
                total = jnp.exp(sink - top) + jnp.sum(exponent, axis=1, keepdims=True)
                shares = (exponent * (1.0 / total)).astype(jnp.bfloat16)
                part = jnp.dot(shares, vals, preferred_element_type=jnp.float32)
                total_out = part if total_out is None else total_out + part
            att[pl.ds(start, WINDOW_REACH), j * LANES : (j + 1) * LANES] = total_out.astype(
                jnp.bfloat16
            )

        @pl.when(n == steps // 2 + 1)
        def _():
            arrive_x(0, 0)

        return carry

    steps = tokens // WINDOW_REACH
    lax.fori_loop(0, steps, attend, 0)

    mine_at = pl.multiple_of(y * rows, rows)
    theirs_at = pl.multiple_of((1 - y) * rows, rows)
    swap = remote(att.at[pl.ds(theirs_at, rows), :], oth, y_sem.at[0], y_sem.at[1], y_peer)
    swap.start()
    for h in range(2):
        x_exchange(1, h).start()
    arrive_x(0, 1)
    arrive(0, 2)
    for load in loads[3:6]:
        load.wait()
    swap.wait_recv()

    me_p = x * n_y + y
    x_p, y_p, d_p = (1 - x) * n_y + y, x * n_y + 1 - y, (1 - x) * n_y + 1 - y
    chunk = 2 * wide

    def row_part(p, h):
        return rows_all.at[pl.ds(pl.multiple_of(p * rows + h * half, half), half), :]

    def give(p, h, way):
        ref = row_part(p, h)
        return remote(ref, ref, g_send.at[0], g_recv.at[p * 2 + h], x_peer if way == 0 else y_peer)

    for h in range(2):
        own_rows = pl.ds(pl.multiple_of(mine_at + h * half, half), half)

        def project(n, square):
            cols = pl.ds(pl.multiple_of(n * chunk, chunk), chunk)
            acc = jnp.dot(
                att[own_rows, :], outw[pl.ds(pl.multiple_of(y * width, width), width), cols],
                preferred_element_type=jnp.float32,
            ) + jnp.dot(
                oth[h * half : (h + 1) * half, :],
                outw[pl.ds(pl.multiple_of((1 - y) * width, width), width), cols],
                preferred_element_type=jnp.float32,
            )
            sums = res[h * half : (h + 1) * half, cols].astype(jnp.float32) + acc.astype(
                jnp.bfloat16
            ).astype(jnp.float32)
            sums = sums.astype(jnp.bfloat16)
            mixed[h * half : (h + 1) * half, cols] = sums
            sums = sums.astype(jnp.float32)
            return square + jnp.sum(sums * sums, axis=1, keepdims=True)

        square = lax.fori_loop(0, model // chunk, project, jnp.zeros((half, 1), jnp.float32))
        scale = lax.rsqrt(square * (1.0 / model) + epsilon)

        def normalise(n, carry):
            cols = pl.ds(pl.multiple_of(n * chunk, chunk), chunk)
            wide_rows = mixed[h * half : (h + 1) * half, cols].astype(jnp.float32)
            rows_all[pl.ds(pl.multiple_of(me_p * rows + h * half, half), half), cols] = (
                wide_rows * scale * gain_ref[:, cols]
            ).astype(jnp.bfloat16)
            return carry

        lax.fori_loop(0, model // chunk, normalise, 0)
        give(me_p, h, 0).start()
        give(me_p, h, 1).start()

    arrive(0, 3)
    n_items = 2 * n_z

    def more(first, until):
        for t in range(first, min(until, n_items)):
            arrive(0, t)

    more(4, 6)
    give(x_p, 0, 0).wait_recv()
    give(x_p, 0, 1).start()
    more(6, 7)
    give(y_p, 1, 1).wait_recv()
    give(y_p, 1, 0).start()
    more(7, n_items)

    own_load(1).wait()
    pass_on(1, 0)
    for h in range(2):
        arrive_x(1, h)

    give(x_p, 1, 0).wait_recv()
    give(y_p, 0, 1).wait_recv()
    give(d_p, 0, 1).wait_recv()
    give(d_p, 1, 0).wait_recv()

    to_core_all(0).wait_recv()
    tall = 2 * rows

    def up_step(i, carry):
        r = pl.ds(pl.multiple_of((i // (quarter // chunk)) * tall, tall), tall)
        f = pl.ds(pl.multiple_of(lax.rem(i, quarter // chunk) * chunk, chunk), chunk)
        before = jnp.dot(rows_all[r, :], up_all[:, f], preferred_element_type=jnp.float32)
        before = jnp.maximum(before, 0.0)
        hid_all[r, f] = (before * before).astype(jnp.bfloat16)
        return carry

    lax.fori_loop(0, 2 * (quarter // chunk), up_step, 0)

    def lanes(ref, h):
        if h is None:
            return ref
        cut = pl.ds(h * blk, blk)
        return ref.at[:, cut] if len(ref.shape) == 2 else ref.at[:, :, cut]

    def partial_slot(j, h):
        return 2 * n_z + lax.rem(j, n_x) if h == 0 else j

    def way(s):
        return jnp.where(s >= 2, 1 - x, x), jnp.where(lax.rem(s, 2) == 1, 1 - y, y)

    def partial_copy(j, s, h=None):
        px, py = way(s)
        return remote(
            lanes(psend.at[j, s - 1], h), lanes(precv.at[j, s - 1], h),
            p_send.at[0], p_recv.at[partial_slot(j, h)], at(z, px, py, c),
        )

    def partials(j, h=None):
        return remote(
            lanes(psend.at[j], h), lanes(precv.at[j], h),
            p_send.at[0], p_recv.at[partial_slot(j, h)], x_peer,
        )

    def pair_of(t):
        zb, b, xb = place(t)
        return zb * n_x + xb

    def combine(t, h=None):
        j = pair_of(t)
        total = lanes(own_sum.at[j], h)[...]
        partials(j, h).wait_recv()
        for s in (1, 2, 3):
            total = total + lanes(precv.at[j, s - 1], h)[...].astype(jnp.float32)
        size = wide if h is None else blk
        cols = pl.ds(pl.multiple_of(j * wide + (h or 0) * blk, blk), size)
        out_ref[:, cols] = (
            mixed[:, cols].astype(jnp.float32) + total.astype(jnp.bfloat16).astype(jnp.float32)
        ).astype(jnp.bfloat16)

    def pieces(j, h=None):
        def piece(i, carry):
            s = 3 - i
            px, py = way(s)
            first = pl.multiple_of((px * n_y + py) * rows, rows)
            part = jnp.dot(
                hid_all[pl.ds(first, rows), :], lanes(down_all.at[j], h)[...],
                preferred_element_type=jnp.float32,
            )

            @pl.when(s > 0)
            def _():
                lanes(psend.at[j, s - 1], h)[...] = part.astype(jnp.bfloat16)
                partial_copy(j, s, h).start()

            @pl.when(s == 0)
            def _():
                lanes(own_sum.at[j], h)[...] = part

            return carry

        lax.fori_loop(0, n_x * n_y, piece, 0)

    lag = 4
    n_whole = n_items - 2

    def line_sent(phase):
        for here in range(n_z):
            blocks = 2 * (here + 1) * (here < n_z - 1) + 2 * (n_z - here) * (here > 0)

            @pl.when(z == here)
            def _():
                if phase == 0:
                    ref = up_all.at[pl.ds(0, blocks * blk), :]
                else:
                    ref = down_all.at[pl.ds(0, blocks // 2)]
                remote(ref, ref, z_send.at[phase], z_recv.at[phase, 0, 0], x_peer).wait_send()

    @pl.when(sp < n_sp - 1)
    def _():
        for i in range(3):
            halo(i).wait_send()

    swap.wait_send()
    for phase in range(2):
        whole = block(phase, z, x, c)
        remote(whole, whole, xs_sem.at[phase], xr_sem.at[phase, 0], x_peer).wait_send()

    def down_step(t, carry):
        @pl.when(t >= 2)
        def _():
            arrive(1, t)

        zb, b, xb = place(t)
        to_core(1, zb, b, xb).wait_recv()
        pieces(pair_of(t))

        @pl.when(t >= lag)
        def _():
            combine(t - lag)

        return carry

    lax.fori_loop(0, n_whole, down_step, 0)

    def last_step(t, carry):
        for h in (1, 0):
            @pl.when(c == h)
            def _():
                arrive(1, t)

            @pl.when(c != h)
            def _():
                zb, b, xb = place(t)
                to_core(1, zb, b, xb).wait_recv()

            pieces(pair_of(t), h)
            done = n_whole - lag + 2 * (t - n_whole) + 1 - h

            @pl.when(done < n_whole - 1)
            def _():
                combine(done)

        return carry

    line_sent(0)
    lax.fori_loop(n_whole, n_items, last_step, 0)
    given = rows_all.at[pl.ds(0, 3 * rows), :]
    remote(given, given, g_send.at[0], g_recv.at[0], x_peer).wait_send()
    line_sent(1)
    for phase in range(2):
        to_core_all(phase).wait_send()

    for t in range(n_whole - 1, n_items):
        for h in (None,) if t < n_whole else (1, 0):
            combine(jnp.int32(t), h)

    remote(psend, precv, p_send.at[0], p_recv.at[0], x_peer).wait_send()


def kernel_body(
    n_z, queries, keys, values, documents, sinks, out_weight, residual, norm_gain, up_weight, down_weight
):
    tokens, width = queries.shape
    rows, model = residual.shape
    blk, hidden = up_weight.shape
    quarter = hidden // 2
    group = 4 * rows
    pairs = 2 * n_z
    bf16, f32 = jnp.bfloat16, jnp.float32
    hbm = pl.BlockSpec(memory_space=pl.ANY)
    dma = pltpu.SemaphoreType.DMA
    return pl.pallas_call(
        functools.partial(layer_kernel, n_z),
        out_shape=pltpu.VMEM((rows, model), bf16),
        in_specs=[hbm] * 10,
        out_specs=pl.BlockSpec(memory_space=pltpu.VMEM),
        scratch_shapes=[
            pltpu.VMEM((model, quarter), bf16),
            pltpu.VMEM((pairs, quarter, 2 * blk), bf16),
            pltpu.VMEM((group, model), bf16),
            pltpu.VMEM((group, quarter), bf16),
            pltpu.VMEM(out_weight.shape, bf16),
            pltpu.VMEM((rows, model), bf16),
            pltpu.VMEM((rows, model), bf16),
            pltpu.VMEM((tokens, width), bf16),
            pltpu.VMEM((tokens + WINDOW_REACH, LANES), bf16),
            pltpu.VMEM((tokens + WINDOW_REACH, LANES), bf16),
            pltpu.VMEM((tokens // LANES + 1, 1, LANES), jnp.int32),
            pltpu.VMEM((tokens,), jnp.int32),
            pltpu.VMEM((tokens,), jnp.int32),
            pltpu.SMEM(sinks.shape, f32),
            pltpu.VMEM((1, model), f32),
            pltpu.VMEM((4, tokens + WINDOW_REACH, LANES), bf16),
            pltpu.VMEM((4, tokens + WINDOW_REACH, LANES), bf16),
            pltpu.VMEM((tokens, width), bf16),
            pltpu.VMEM((rows, width), bf16),
            pltpu.VMEM((pairs, 3, rows, 2 * blk), bf16),
            pltpu.VMEM((pairs, 3, rows, 2 * blk), bf16),
            pltpu.VMEM((pairs, rows, 2 * blk), f32),
            dma((8,)), dma((3,)), dma((3,)), dma((2,)), dma((2, 2)), dma((2,)), dma((2, n_z, 2)),
            dma((2,)), dma((1 + 2 * n_z,)), dma((2,)), dma((1,)), dma((8,)),
            dma((1,)), dma((pairs + 2,)), dma((2,)),
        ],
        compiler_params=pltpu.CompilerParams(collective_id=0, has_side_effects=True, vmem_limit_bytes=60 << 20),
    )(
        queries, keys, values, documents, sinks, out_weight,
        residual, norm_gain.reshape(1, model), up_weight, down_weight,
    )


def body(n_z, mesh, *arrays):
    queries, keys, up_weight, residual = arrays[0], arrays[1], arrays[8], arrays[6]
    if fits(mesh, *queries.shape, keys.shape[1], residual.shape[1], up_weight.shape[1]):
        return kernel_body(n_z, *arrays)
    return gathered_body(*arrays)


def solution(mesh):
    in_specs = (
        P("sp", "tp"),
        P("sp", "tp"),
        P("sp", "tp"),
        P("sp"),
        P("tp"),
        P(),
        P(("sp", "tp"), None),
        P(),
        P("sp", "tp"),
        P("tp", "sp"),
    )
    out_specs = P(("sp", "tp"), None)
    n_z = mesh.shape["sp"] // (CORES * mesh.shape["tp"])
    return jax.shard_map(
        functools.partial(body, n_z, mesh), mesh=mesh, in_specs=in_specs, out_specs=out_specs, check_vma=False
    )
```

```python
import functools

import jax
import jax.numpy as jnp
from jax import lax
from jax.experimental import pallas as pl
from jax.experimental.pallas import tpu as pltpu
from jax.sharding import PartitionSpec as P

HEAD_SIZE = 64
WINDOW_REACH = 128
LANES = 128
CORES = 2
MESH = pl.DeviceIdType.MESH

masked_score = -1e30
epsilon = 1e-06


def passed_along(shard, axis, by):
    peers = lax.axis_size(axis)
    pairs = [(i, i + by) for i in range(peers) if 0 <= i + by < peers]
    return lax.ppermute(shard, axis, pairs)


def rounded(value):
    return lax.optimization_barrier(value.astype(jnp.bfloat16))


def squared_relu(before):
    return jnp.square(jax.nn.relu(before)).astype(jnp.bfloat16)


def windowed_attention(queries, keys, values, documents, sinks):
    length = queries.shape[0]
    heads = queries.shape[1] // HEAD_SIZE
    kv_heads = keys.shape[1] // HEAD_SIZE
    query_group = heads // kv_heads
    block_list = length // WINDOW_REACH
    prev_keys, prev_values, prev_docs = passed_along(
        (
            keys[length - WINDOW_REACH :],
            values[length - WINDOW_REACH :],
            documents[length - WINDOW_REACH :],
        ),
        "sp",
        1,
    )
    offset = lax.axis_index("sp") * length
    key_matrix = jnp.concatenate([prev_keys, keys], axis=0).reshape(
        block_list + 1, WINDOW_REACH, kv_heads, HEAD_SIZE
    )
    value_matrix = jnp.concatenate([prev_values, values], axis=0).reshape(
        block_list + 1, WINDOW_REACH, kv_heads, HEAD_SIZE
    )
    key_docs = jnp.concatenate([prev_docs, documents], axis=0).reshape(block_list + 1, WINDOW_REACH)
    key_place = (
        offset - WINDOW_REACH + jnp.arange((block_list + 1) * WINDOW_REACH, dtype=jnp.int32)
    ).reshape(block_list + 1, WINDOW_REACH)
    band_keys = jnp.concatenate([key_matrix[:-1], key_matrix[1:]], axis=1)
    band_values = jnp.concatenate([value_matrix[:-1], value_matrix[1:]], axis=1)
    band_docs = jnp.concatenate([key_docs[:-1], key_docs[1:]], axis=1)
    band_place = jnp.concatenate([key_place[:-1], key_place[1:]], axis=1)
    query_docs = documents.reshape(block_list, WINDOW_REACH)
    grouped_queries = queries.reshape(block_list, WINDOW_REACH, kv_heads, query_group, HEAD_SIZE)
    scores = jnp.einsum(
        "nqhgd,nshd->nhgqs", grouped_queries, band_keys, preferred_element_type=jnp.float32
    ) * HEAD_SIZE ** (-0.5)
    row_index = jnp.arange(WINDOW_REACH, dtype=jnp.int32)[:, None]
    col_index = jnp.arange(2 * WINDOW_REACH, dtype=jnp.int32)[None, :]
    distance = WINDOW_REACH + row_index - col_index
    near = (distance >= 0) & (distance < WINDOW_REACH)
    visible = (
        near[None]
        & (band_docs[:, None, :] == query_docs[:, :, None])
        & (band_place[:, None, :] >= 0)
    )
    visible = visible[:, None, None]
    head_sink_logit = sinks.reshape(kv_heads, query_group)[None, :, :, None]
    scores = jnp.where(visible, scores, masked_score)
    top = jnp.maximum(jnp.max(scores, axis=-1), head_sink_logit)
    exponent = jnp.where(visible, jnp.exp(scores - top[..., None]), 0.0)
    total = jnp.exp(head_sink_logit - top) + jnp.sum(exponent, axis=-1)
    shares = (exponent / total[..., None]).astype(jnp.bfloat16)
    attended = jnp.einsum(
        "nhgqs,nshd->nqhgd", shares, band_values, preferred_element_type=jnp.float32
    )
    return attended.astype(jnp.bfloat16).reshape(length, heads * HEAD_SIZE)


def rotated(shard, axis, by):
    peers = lax.axis_size(axis)
    return lax.ppermute(shard, axis, [(i, (i + by) % peers) for i in range(peers)])


def row_block(array, index, rows):
    return lax.dynamic_slice_in_dim(array, index * rows, rows, axis=0)


def gathered_body(
    queries, keys, values, documents, sinks, out_weight, residual, norm_gain, up_weight, down_weight
):
    up_whole, down_whole = (
        lax.all_gather(up_weight, "sp", axis=0, tiled=True),
        lax.all_gather(down_weight, "sp", axis=1, tiled=True),
    )
    n_tp = lax.axis_size("tp")
    me = lax.axis_index("tp")
    rows = residual.shape[0]
    attended = windowed_attention(queries, keys, values, documents, sinks)
    width = attended.shape[1]
    token_heads = jnp.zeros((rows, width * n_tp), jnp.bfloat16)
    for by in range(n_tp):
        piece = row_block(attended, (me + by) % n_tp, rows)
        if by:
            piece = rotated(piece, "tp", by)
        token_heads = lax.dynamic_update_slice_in_dim(
            token_heads, piece, ((me - by) % n_tp) * width, axis=1
        )
    projected = jnp.dot(token_heads, out_weight, preferred_element_type=jnp.float32)
    mixed = rounded(residual.astype(jnp.float32) + rounded(projected).astype(jnp.float32))
    widened = mixed.astype(jnp.float32)
    normed = (
        widened
        * lax.rsqrt(jnp.mean(widened * widened, axis=-1, keepdims=True) + epsilon)
        * norm_gain
    ).astype(jnp.bfloat16)
    branch = 0.0
    for by in range(n_tp - 1, -1, -1):
        rows_in = rotated(normed, "tp", by) if by else normed
        hidden = squared_relu(jnp.dot(rows_in, up_whole, preferred_element_type=jnp.float32))
        partial = jnp.dot(hidden, down_whole, preferred_element_type=jnp.float32).astype(
            jnp.bfloat16
        )
        if by:
            partial = rotated(partial, "tp", n_tp - by)
        branch = branch + partial.astype(jnp.float32)
    return (widened + rounded(branch).astype(jnp.float32)).astype(jnp.bfloat16)


def fits(mesh, tokens, width, kv_width, model, hidden):
    n_sp, n_tp = mesh.shape["sp"], mesh.shape["tp"]
    block = model // n_sp
    return (
        n_tp == 2
        and n_sp % (n_tp * CORES) == 0
        and n_sp // (n_tp * CORES) >= 3
        and block % LANES == 0
        and kv_width == LANES
        and width % (2 * LANES) == 0
        and tokens % (2 * WINDOW_REACH // 2) == 0
        and (tokens // n_tp) % 32 == 0
        and hidden % (n_tp * 2 * LANES) == 0
    )


def layer_kernel(
    n_z,
    q_hbm, k_hbm, v_hbm, docs_hbm, sinks_hbm, outw_hbm, res_hbm, gain_hbm, up_hbm, down_hbm,
    out_ref,
    up_all, down_all, rows_all, hid_all, outw, res, mixed, q_ref, k_ref, v_ref, docs, docs_prev, docs_flat, sinks, gain_ref,
    k_wide, v_wide, att, oth, psend, precv, own_sum,
    load_sem, halo_send, halo_recv, xs_sem, xr_sem, z_send, z_recv, d_send, d_recv, y_sem,
    g_send, g_recv, p_send, p_recv, own_sem,
):
    sp, y = lax.axis_index("sp"), lax.axis_index("tp")
    n_x, n_y = 2, 2
    z, x, c = sp // (n_x * CORES), lax.rem(sp // CORES, n_x), lax.rem(sp, CORES)
    n_sp = n_z * n_x * CORES
    tokens = q_ref.shape[0]
    rows = res.shape[0]
    half = rows // 2
    model = res.shape[1]
    width = q_ref.shape[1]
    blk = up_hbm.shape[0]
    quarter = up_hbm.shape[1] // n_x
    wide = 2 * blk

    def at(zz, xx, yy, cc):
        return ((zz * n_x + xx) * CORES + cc, yy)

    def remote(src, dst, send, recv, dev):
        return pltpu.make_async_remote_copy(
            src_ref=src, dst_ref=dst, send_sem=send, recv_sem=recv, device_id=dev, device_id_type=MESH
        )

    x_peer, y_peer, c_peer = at(z, 1 - x, y, c), at(z, x, 1 - y, c), at(z, x, y, 1 - c)

    def block(phase, zb, xb, cb):
        if phase == 0:
            first = ((zb * n_x + xb) * CORES + cb) * blk
            return up_all.at[pl.ds(pl.multiple_of(first, blk), blk), :]
        return down_all.at[zb * n_x + xb, :, pl.ds(pl.multiple_of(cb * blk, blk), blk)]

    def own_piece(phase, xq):
        start = pl.multiple_of(xq * quarter, quarter)
        if phase == 0:
            return up_hbm.at[:, pl.ds(start, quarter)]
        return down_hbm.at[pl.ds(start, quarter), :]

    def part_of(ref, h):
        size = ref.shape[0] // 2
        return ref.at[pl.ds(h * size, size), :]

    def x_exchange(phase, h):
        return remote(
            part_of(own_piece(phase, 1 - x), h), part_of(block(phase, z, x, c), h),
            xs_sem.at[phase], xr_sem.at[phase, h], x_peer,
        )

    def own_load(phase):
        return pltpu.make_async_copy(own_piece(phase, x), block(phase, z, x, c), own_sem.at[phase])

    low = jnp.minimum(z, n_z - 1 - z)
    inward = jnp.where(2 * z < n_z, 1, -1)

    def plane(k):
        near = z + jnp.where(lax.rem(k, 2) == 1, inward, -inward) * ((k + 1) // 2)
        far = jnp.where(z < n_z - 1 - z, k, n_z - 1 - k)
        return jnp.where(k <= 2 * low, near, far)

    def place(t):
        zb, b = plane(t // 2), lax.rem(t, 2)
        return zb, b, jnp.where(b == 0, x, 1 - x)

    def to_up(phase, zb, b, xb):
        ref = block(phase, zb, xb, c)
        return remote(ref, ref, z_send.at[phase], z_recv.at[phase, zb, b], at(z + 1, x, y, c))

    def to_down(phase, zb, b, xb):
        ref = block(phase, zb, xb, c)
        return remote(ref, ref, z_send.at[phase], z_recv.at[phase, zb, b], at(z - 1, x, y, c))

    def to_core(phase, zb, b, xb):
        ref = block(phase, zb, xb, c)
        slot = 0 if phase == 0 else 1 + zb * n_x + b
        return remote(ref, ref, d_send.at[phase], d_recv.at[slot], c_peer)

    def to_core_all(phase):
        ref = up_all.at[pl.ds(0, model // 2), :] if phase == 0 else down_all.at[pl.ds(0, n_z)]
        return remote(ref, ref, d_send.at[phase], d_recv.at[0], c_peer)

    def goes_up(zb):
        return jnp.logical_and(zb <= z, z < n_z - 1)

    def goes_down(zb):
        return jnp.logical_and(zb >= z, z > 0)

    def pass_on(phase, t):
        zb, b, xb = place(t)

        @pl.when(goes_up(zb))
        def _():
            to_up(phase, zb, b, xb).start()

        @pl.when(goes_down(zb))
        def _():
            to_down(phase, zb, b, xb).start()

        to_core(phase, zb, b, xb).start()

    def arrive_x(phase, h):
        x_exchange(phase, h).wait_recv()
        ref = part_of(block(phase, z, 1 - x, c), h)

        @pl.when(z < n_z - 1)
        def _():
            remote(
                ref, ref, z_send.at[phase], z_recv.at[phase, z, 1], at(z + 1, x, y, c)
            ).start()

        @pl.when(z > 0)
        def _():
            remote(
                ref, ref, z_send.at[phase], z_recv.at[phase, z, 1], at(z - 1, x, y, c)
            ).start()

        if h == 1:
            to_core(phase, z, 1, 1 - x).start()

    def arrive(phase, t):
        zb, b, xb = place(t)
        to_up(phase, zb, b, xb).wait_recv()
        pass_on(phase, t)

    last = tokens - WINDOW_REACH
    nxt = (sp + 1, y)

    def halo(i):
        src, dst = (
            (k_hbm.at[pl.ds(last, WINDOW_REACH), :], k_ref.at[pl.ds(0, WINDOW_REACH), :]),
            (v_hbm.at[pl.ds(last, WINDOW_REACH), :], v_ref.at[pl.ds(0, WINDOW_REACH), :]),
            (docs_hbm, docs_prev),
        )[i]
        return remote(src, dst, halo_send.at[i], halo_recv.at[i], nxt)

    own_load(0).start()
    barrier = pltpu.get_barrier_semaphore()
    partners = (
        (True, x_peer), (True, y_peer), (True, at(z, 1 - x, 1 - y, c)), (True, c_peer),
        (z < n_z - 1, at(z + 1, x, y, c)), (z > 0, at(z - 1, x, y, c)),
        (sp < n_sp - 1, nxt), (sp > 0, (sp - 1, y)),
    )
    for here, dev in partners:
        @pl.when(here)
        def _():
            pl.semaphore_signal(barrier, inc=1, device_id=dev, device_id_type=MESH)

    pl.semaphore_wait(barrier, sum(jnp.int32(here) for here, _ in partners))

    @pl.when(sp < n_sp - 1)
    def _():
        for i in range(3):
            halo(i).start()

    loads = [
        pltpu.make_async_copy(q_hbm, q_ref, load_sem.at[0]),
        pltpu.make_async_copy(k_hbm, k_ref.at[pl.ds(WINDOW_REACH, tokens), :], load_sem.at[1]),
        pltpu.make_async_copy(v_hbm, v_ref.at[pl.ds(WINDOW_REACH, tokens), :], load_sem.at[2]),
        pltpu.make_async_copy(outw_hbm, outw, load_sem.at[3]),
        pltpu.make_async_copy(res_hbm, res, load_sem.at[4]),
        pltpu.make_async_copy(gain_hbm, gain_ref, load_sem.at[5]),
        pltpu.make_async_copy(docs_hbm, docs_flat, load_sem.at[6]),
        pltpu.make_async_copy(sinks_hbm, sinks, load_sem.at[7]),
    ]
    own_load(0).wait()

    def begin():
        x_exchange(0, 0).start()
        pass_on(0, 0)
        x_exchange(0, 1).start()

    @pl.when(c == 1)
    def _():
        begin()

    for load in loads:
        load.start()
    own_load(1).start()

    @pl.when(sp == 0)
    def _():
        k_ref[pl.ds(0, WINDOW_REACH), :] = jnp.zeros((WINDOW_REACH, LANES), jnp.bfloat16)
        v_ref[pl.ds(0, WINDOW_REACH), :] = jnp.zeros((WINDOW_REACH, LANES), jnp.bfloat16)
        docs_prev[...] = jnp.full(docs_prev.shape, -1, jnp.int32)

    for load in loads[:3] + loads[6:]:
        load.wait()

    @pl.when(sp > 0)
    def _():
        for i in range(3):
            halo(i).wait_recv()

    docs[0, 0] = docs_prev[last:]
    for i in range(tokens // LANES):
        docs[i + 1, 0] = docs_flat[i * LANES : (i + 1) * LANES]
    @pl.when(c == 0)
    def _():
        begin()

    heads = width // HEAD_SIZE
    kv_heads = LANES // HEAD_SIZE
    group = heads // kv_heads
    lane_in = lax.broadcasted_iota(jnp.int32, (LANES, LANES), 0)
    lane_out = lax.broadcasted_iota(jnp.int32, (LANES, LANES), 1)
    for g in range(kv_heads):
        for par in range(2):
            pick = (lane_in - g * HEAD_SIZE == lane_out - par * HEAD_SIZE) & (
                lane_out // HEAD_SIZE == par
            )
            pick = pick.astype(jnp.float32).astype(jnp.bfloat16)
            for raw, spread in ((k_ref, k_wide), (v_ref, v_wide)):
                spread[g * 2 + par] = jnp.dot(
                    raw[...], pick, preferred_element_type=jnp.float32
                ).astype(jnp.bfloat16)

    row_i = lax.broadcasted_iota(jnp.int32, (WINDOW_REACH, 2 * WINDOW_REACH), 0)
    col_i = lax.broadcasted_iota(jnp.int32, (WINDOW_REACH, 2 * WINDOW_REACH), 1)
    near = (col_i > row_i) & (col_i <= row_i + WINDOW_REACH)

    def attend(n, carry):
        start = pl.multiple_of(n * WINDOW_REACH, WINDOW_REACH)
        early = jnp.broadcast_to(docs[n], (WINDOW_REACH, LANES))
        late = jnp.broadcast_to(docs[n + 1], (WINDOW_REACH, LANES))
        mine = late.T
        same = jnp.concatenate([early == mine, late == mine], axis=1)
        visible = near & same
        for j in range(width // LANES):
            total_out = None
            g = (2 * j) // group
            q_blk = q_ref[pl.ds(start, WINDOW_REACH), j * LANES : (j + 1) * LANES]
            for par in range(2):
                head = 2 * j + par
                keys = k_wide[g * 2 + par, pl.ds(start, 2 * WINDOW_REACH), :]
                vals = v_wide[g * 2 + par, pl.ds(start, 2 * WINDOW_REACH), :]
                scores = lax.dot_general(
                    q_blk, keys, (((1,), (1,)), ((), ())), preferred_element_type=jnp.float32
                ) * HEAD_SIZE ** (-0.5)
                scores = jnp.where(visible, scores, masked_score)
                sink = sinks[head]
                top = jnp.maximum(jnp.max(scores, axis=1, keepdims=True), sink)
                exponent = jnp.where(visible, jnp.exp(scores - top), 0.0)
                total = jnp.exp(sink - top) + jnp.sum(exponent, axis=1, keepdims=True)
                shares = (exponent * (1.0 / total)).astype(jnp.bfloat16)
                part = jnp.dot(shares, vals, preferred_element_type=jnp.float32)
                total_out = part if total_out is None else total_out + part
            att[pl.ds(start, WINDOW_REACH), j * LANES : (j + 1) * LANES] = total_out.astype(
                jnp.bfloat16
            )

        @pl.when(n == steps // 2 + 1)
        def _():
            arrive_x(0, 0)

        return carry

    steps = tokens // WINDOW_REACH
    lax.fori_loop(0, steps, attend, 0)

    mine_at = pl.multiple_of(y * rows, rows)
    theirs_at = pl.multiple_of((1 - y) * rows, rows)
    swap = remote(att.at[pl.ds(theirs_at, rows), :], oth, y_sem.at[0], y_sem.at[1], y_peer)
    swap.start()
    for h in range(2):
        x_exchange(1, h).start()
    arrive_x(0, 1)
    arrive(0, 2)
    for load in loads[3:6]:
        load.wait()
    swap.wait_recv()

    me_p = x * n_y + y
    x_p, y_p, d_p = (1 - x) * n_y + y, x * n_y + 1 - y, (1 - x) * n_y + 1 - y
    chunk = 2 * wide

    def row_part(p, h):
        return rows_all.at[pl.ds(pl.multiple_of(p * rows + h * half, half), half), :]

    def give(p, h, way):
        ref = row_part(p, h)
        return remote(ref, ref, g_send.at[0], g_recv.at[p * 2 + h], x_peer if way == 0 else y_peer)

    for h in range(2):
        own_rows = pl.ds(pl.multiple_of(mine_at + h * half, half), half)

        def project(n, square):
            cols = pl.ds(pl.multiple_of(n * chunk, chunk), chunk)
            acc = jnp.dot(
                att[own_rows, :], outw[pl.ds(pl.multiple_of(y * width, width), width), cols],
                preferred_element_type=jnp.float32,
            ) + jnp.dot(
                oth[h * half : (h + 1) * half, :],
                outw[pl.ds(pl.multiple_of((1 - y) * width, width), width), cols],
                preferred_element_type=jnp.float32,
            )
            sums = res[h * half : (h + 1) * half, cols].astype(jnp.float32) + acc.astype(
                jnp.bfloat16
            ).astype(jnp.float32)
            sums = sums.astype(jnp.bfloat16)
            mixed[h * half : (h + 1) * half, cols] = sums
            sums = sums.astype(jnp.float32)
            return square + jnp.sum(sums * sums, axis=1, keepdims=True)

        square = lax.fori_loop(0, model // chunk, project, jnp.zeros((half, 1), jnp.float32))
        scale = lax.rsqrt(square * (1.0 / model) + epsilon)

        def normalise(n, carry):
            cols = pl.ds(pl.multiple_of(n * chunk, chunk), chunk)
            wide_rows = mixed[h * half : (h + 1) * half, cols].astype(jnp.float32)
            rows_all[pl.ds(pl.multiple_of(me_p * rows + h * half, half), half), cols] = (
                wide_rows * scale * gain_ref[:, cols]
            ).astype(jnp.bfloat16)
            return carry

        lax.fori_loop(0, model // chunk, normalise, 0)
        give(me_p, h, 0).start()
        give(me_p, h, 1).start()

    arrive(0, 3)
    n_items = 2 * n_z

    def more(first, until):
        for t in range(first, min(until, n_items)):
            arrive(0, t)

    more(4, 6)
    give(x_p, 0, 0).wait_recv()
    give(x_p, 0, 1).start()
    more(6, 7)
    give(y_p, 1, 1).wait_recv()
    give(y_p, 1, 0).start()
    more(7, n_items)

    own_load(1).wait()
    pass_on(1, 0)
    for h in range(2):
        arrive_x(1, h)

    give(x_p, 1, 0).wait_recv()
    give(y_p, 0, 1).wait_recv()
    give(d_p, 0, 1).wait_recv()
    give(d_p, 1, 0).wait_recv()

    to_core_all(0).wait_recv()
    tall = 2 * rows

    def up_step(i, carry):
        r = pl.ds(pl.multiple_of((i // (quarter // chunk)) * tall, tall), tall)
        f = pl.ds(pl.multiple_of(lax.rem(i, quarter // chunk) * chunk, chunk), chunk)
        before = jnp.dot(rows_all[r, :], up_all[:, f], preferred_element_type=jnp.float32)
        before = jnp.maximum(before, 0.0)
        hid_all[r, f] = (before * before).astype(jnp.bfloat16)
        return carry

    lax.fori_loop(0, 2 * (quarter // chunk), up_step, 0)

    def lanes(ref, h):
        if h is None:
            return ref
        cut = pl.ds(h * blk, blk)
        return ref.at[:, cut] if len(ref.shape) == 2 else ref.at[:, :, cut]

    def partial_slot(j, h):
        return 2 * n_z + lax.rem(j, n_x) if h == 0 else j

    def way(s):
        return jnp.where(s >= 2, 1 - x, x), jnp.where(lax.rem(s, 2) == 1, 1 - y, y)

    def partial_copy(j, s, h=None):
        px, py = way(s)
        return remote(
            lanes(psend.at[j, s - 1], h), lanes(precv.at[j, s - 1], h),
            p_send.at[0], p_recv.at[partial_slot(j, h)], at(z, px, py, c),
        )

    def partials(j, h=None):
        return remote(
            lanes(psend.at[j], h), lanes(precv.at[j], h),
            p_send.at[0], p_recv.at[partial_slot(j, h)], x_peer,
        )

    def pair_of(t):
        zb, b, xb = place(t)
        return zb * n_x + xb

    def combine(t, h=None):
        j = pair_of(t)
        total = lanes(own_sum.at[j], h)[...]
        partials(j, h).wait_recv()
        for s in (1, 2, 3):
            total = total + lanes(precv.at[j, s - 1], h)[...].astype(jnp.float32)
        size = wide if h is None else blk
        cols = pl.ds(pl.multiple_of(j * wide + (h or 0) * blk, blk), size)
        out_ref[:, cols] = (
            mixed[:, cols].astype(jnp.float32) + total.astype(jnp.bfloat16).astype(jnp.float32)
        ).astype(jnp.bfloat16)

    def pieces(j, h=None):
        def piece(i, carry):
            s = jnp.where(i == 0, 1, jnp.where(i == 1, 3, jnp.where(i == 2, 2, 0)))
            px, py = way(s)
            first = pl.multiple_of((px * n_y + py) * rows, rows)
            part = jnp.dot(
                hid_all[pl.ds(first, rows), :], lanes(down_all.at[j], h)[...],
                preferred_element_type=jnp.float32,
            )

            @pl.when(s > 0)
            def _():
                lanes(psend.at[j, s - 1], h)[...] = part.astype(jnp.bfloat16)
                partial_copy(j, s, h).start()

            @pl.when(s == 0)
            def _():
                lanes(own_sum.at[j], h)[...] = part

            return carry

        lax.fori_loop(0, n_x * n_y, piece, 0)

    lag = 4
    n_whole = n_items - 2

    def line_sent(phase):
        for here in range(n_z):
            blocks = 2 * (here + 1) * (here < n_z - 1) + 2 * (n_z - here) * (here > 0)

            @pl.when(z == here)
            def _():
                if phase == 0:
                    ref = up_all.at[pl.ds(0, blocks * blk), :]
                else:
                    ref = down_all.at[pl.ds(0, blocks // 2)]
                remote(ref, ref, z_send.at[phase], z_recv.at[phase, 0, 0], x_peer).wait_send()

    @pl.when(sp < n_sp - 1)
    def _():
        for i in range(3):
            halo(i).wait_send()

    swap.wait_send()
    for phase in range(2):
        whole = block(phase, z, x, c)
        remote(whole, whole, xs_sem.at[phase], xr_sem.at[phase, 0], x_peer).wait_send()

    def down_step(t, carry):
        @pl.when(t >= 2)
        def _():
            arrive(1, t)

        zb, b, xb = place(t)
        to_core(1, zb, b, xb).wait_recv()
        pieces(pair_of(t))

        @pl.when(t >= lag)
        def _():
            combine(t - lag)

        return carry

    lax.fori_loop(0, n_whole, down_step, 0)

    def last_step(t, carry):
        for h in (1, 0):
            @pl.when(c == h)
            def _():
                arrive(1, t)

            @pl.when(c != h)
            def _():
                zb, b, xb = place(t)
                to_core(1, zb, b, xb).wait_recv()

            pieces(pair_of(t), h)
            done = n_whole - lag + 2 * (t - n_whole) + 1 - h

            @pl.when(done < n_whole - 1)
            def _():
                combine(done)

        return carry

    line_sent(0)
    lax.fori_loop(n_whole, n_items, last_step, 0)
    given = rows_all.at[pl.ds(0, 3 * rows), :]
    remote(given, given, g_send.at[0], g_recv.at[0], x_peer).wait_send()
    line_sent(1)
    for phase in range(2):
        to_core_all(phase).wait_send()

    for t in range(n_whole - 1, n_items):
        for h in (None,) if t < n_whole else (1, 0):
            combine(jnp.int32(t), h)

    remote(psend, precv, p_send.at[0], p_recv.at[0], x_peer).wait_send()


def kernel_body(
    n_z, queries, keys, values, documents, sinks, out_weight, residual, norm_gain, up_weight, down_weight
):
    tokens, width = queries.shape
    rows, model = residual.shape
    blk, hidden = up_weight.shape
    quarter = hidden // 2
    group = 4 * rows
    pairs = 2 * n_z
    bf16, f32 = jnp.bfloat16, jnp.float32
    hbm = pl.BlockSpec(memory_space=pl.ANY)
    dma = pltpu.SemaphoreType.DMA
    return pl.pallas_call(
        functools.partial(layer_kernel, n_z),
        out_shape=pltpu.VMEM((rows, model), bf16),
        in_specs=[hbm] * 10,
        out_specs=pl.BlockSpec(memory_space=pltpu.VMEM),
        scratch_shapes=[
            pltpu.VMEM((model, quarter), bf16),
            pltpu.VMEM((pairs, quarter, 2 * blk), bf16),
            pltpu.VMEM((group, model), bf16),
            pltpu.VMEM((group, quarter), bf16),
            pltpu.VMEM(out_weight.shape, bf16),
            pltpu.VMEM((rows, model), bf16),
            pltpu.VMEM((rows, model), bf16),
            pltpu.VMEM((tokens, width), bf16),
            pltpu.VMEM((tokens + WINDOW_REACH, LANES), bf16),
            pltpu.VMEM((tokens + WINDOW_REACH, LANES), bf16),
            pltpu.VMEM((tokens // LANES + 1, 1, LANES), jnp.int32),
            pltpu.VMEM((tokens,), jnp.int32),
            pltpu.VMEM((tokens,), jnp.int32),
            pltpu.SMEM(sinks.shape, f32),
            pltpu.VMEM((1, model), f32),
            pltpu.VMEM((4, tokens + WINDOW_REACH, LANES), bf16),
            pltpu.VMEM((4, tokens + WINDOW_REACH, LANES), bf16),
            pltpu.VMEM((tokens, width), bf16),
            pltpu.VMEM((rows, width), bf16),
            pltpu.VMEM((pairs, 3, rows, 2 * blk), bf16),
            pltpu.VMEM((pairs, 3, rows, 2 * blk), bf16),
            pltpu.VMEM((pairs, rows, 2 * blk), f32),
            dma((8,)), dma((3,)), dma((3,)), dma((2,)), dma((2, 2)), dma((2,)), dma((2, n_z, 2)),
            dma((2,)), dma((1 + 2 * n_z,)), dma((2,)), dma((1,)), dma((8,)),
            dma((1,)), dma((pairs + 2,)), dma((2,)),
        ],
        compiler_params=pltpu.CompilerParams(collective_id=0, has_side_effects=True, vmem_limit_bytes=60 << 20),
    )(
        queries, keys, values, documents, sinks, out_weight,
        residual, norm_gain.reshape(1, model), up_weight, down_weight,
    )


def body(n_z, mesh, *arrays):
    queries, keys, up_weight, residual = arrays[0], arrays[1], arrays[8], arrays[6]
    if fits(mesh, *queries.shape, keys.shape[1], residual.shape[1], up_weight.shape[1]):
        return kernel_body(n_z, *arrays)
    return gathered_body(*arrays)


def solution(mesh):
    in_specs = (
        P("sp", "tp"),
        P("sp", "tp"),
        P("sp", "tp"),
        P("sp"),
        P("tp"),
        P(),
        P(("sp", "tp"), None),
        P(),
        P("sp", "tp"),
        P("tp", "sp"),
    )
    out_specs = P(("sp", "tp"), None)
    n_z = mesh.shape["sp"] // (CORES * mesh.shape["tp"])
    return jax.shard_map(
        functools.partial(body, n_z, mesh), mesh=mesh, in_specs=in_specs, out_specs=out_specs, check_vma=False
    )
```

```python
import functools

import jax
import jax.numpy as jnp
from jax import lax
from jax.experimental import pallas as pl
from jax.experimental.pallas import tpu as pltpu
from jax.sharding import PartitionSpec as P

HEAD_SIZE = 64
WINDOW_REACH = 128
LANES = 128
CORES = 2
MESH = pl.DeviceIdType.MESH

masked_score = -1e30
epsilon = 1e-06


def passed_along(shard, axis, by):
    peers = lax.axis_size(axis)
    pairs = [(i, i + by) for i in range(peers) if 0 <= i + by < peers]
    return lax.ppermute(shard, axis, pairs)


def rounded(value):
    return lax.optimization_barrier(value.astype(jnp.bfloat16))


def squared_relu(before):
    return jnp.square(jax.nn.relu(before)).astype(jnp.bfloat16)


def windowed_attention(queries, keys, values, documents, sinks):
    length = queries.shape[0]
    heads = queries.shape[1] // HEAD_SIZE
    kv_heads = keys.shape[1] // HEAD_SIZE
    query_group = heads // kv_heads
    block_list = length // WINDOW_REACH
    prev_keys, prev_values, prev_docs = passed_along(
        (
            keys[length - WINDOW_REACH :],
            values[length - WINDOW_REACH :],
            documents[length - WINDOW_REACH :],
        ),
        "sp",
        1,
    )
    offset = lax.axis_index("sp") * length
    key_matrix = jnp.concatenate([prev_keys, keys], axis=0).reshape(
        block_list + 1, WINDOW_REACH, kv_heads, HEAD_SIZE
    )
    value_matrix = jnp.concatenate([prev_values, values], axis=0).reshape(
        block_list + 1, WINDOW_REACH, kv_heads, HEAD_SIZE
    )
    key_docs = jnp.concatenate([prev_docs, documents], axis=0).reshape(block_list + 1, WINDOW_REACH)
    key_place = (
        offset - WINDOW_REACH + jnp.arange((block_list + 1) * WINDOW_REACH, dtype=jnp.int32)
    ).reshape(block_list + 1, WINDOW_REACH)
    band_keys = jnp.concatenate([key_matrix[:-1], key_matrix[1:]], axis=1)
    band_values = jnp.concatenate([value_matrix[:-1], value_matrix[1:]], axis=1)
    band_docs = jnp.concatenate([key_docs[:-1], key_docs[1:]], axis=1)
    band_place = jnp.concatenate([key_place[:-1], key_place[1:]], axis=1)
    query_docs = documents.reshape(block_list, WINDOW_REACH)
    grouped_queries = queries.reshape(block_list, WINDOW_REACH, kv_heads, query_group, HEAD_SIZE)
    scores = jnp.einsum(
        "nqhgd,nshd->nhgqs", grouped_queries, band_keys, preferred_element_type=jnp.float32
    ) * HEAD_SIZE ** (-0.5)
    row_index = jnp.arange(WINDOW_REACH, dtype=jnp.int32)[:, None]
    col_index = jnp.arange(2 * WINDOW_REACH, dtype=jnp.int32)[None, :]
    distance = WINDOW_REACH + row_index - col_index
    near = (distance >= 0) & (distance < WINDOW_REACH)
    visible = (
        near[None]
        & (band_docs[:, None, :] == query_docs[:, :, None])
        & (band_place[:, None, :] >= 0)
    )
    visible = visible[:, None, None]
    head_sink_logit = sinks.reshape(kv_heads, query_group)[None, :, :, None]
    scores = jnp.where(visible, scores, masked_score)
    top = jnp.maximum(jnp.max(scores, axis=-1), head_sink_logit)
    exponent = jnp.where(visible, jnp.exp(scores - top[..., None]), 0.0)
    total = jnp.exp(head_sink_logit - top) + jnp.sum(exponent, axis=-1)
    shares = (exponent / total[..., None]).astype(jnp.bfloat16)
    attended = jnp.einsum(
        "nhgqs,nshd->nqhgd", shares, band_values, preferred_element_type=jnp.float32
    )
    return attended.astype(jnp.bfloat16).reshape(length, heads * HEAD_SIZE)


def rotated(shard, axis, by):
    peers = lax.axis_size(axis)
    return lax.ppermute(shard, axis, [(i, (i + by) % peers) for i in range(peers)])


def row_block(array, index, rows):
    return lax.dynamic_slice_in_dim(array, index * rows, rows, axis=0)


def gathered_body(
    queries, keys, values, documents, sinks, out_weight, residual, norm_gain, up_weight, down_weight
):
    up_whole, down_whole = (
        lax.all_gather(up_weight, "sp", axis=0, tiled=True),
        lax.all_gather(down_weight, "sp", axis=1, tiled=True),
    )
    n_tp = lax.axis_size("tp")
    me = lax.axis_index("tp")
    rows = residual.shape[0]
    attended = windowed_attention(queries, keys, values, documents, sinks)
    width = attended.shape[1]
    token_heads = jnp.zeros((rows, width * n_tp), jnp.bfloat16)
    for by in range(n_tp):
        piece = row_block(attended, (me + by) % n_tp, rows)
        if by:
            piece = rotated(piece, "tp", by)
        token_heads = lax.dynamic_update_slice_in_dim(
            token_heads, piece, ((me - by) % n_tp) * width, axis=1
        )
    projected = jnp.dot(token_heads, out_weight, preferred_element_type=jnp.float32)
    mixed = rounded(residual.astype(jnp.float32) + rounded(projected).astype(jnp.float32))
    widened = mixed.astype(jnp.float32)
    normed = (
        widened
        * lax.rsqrt(jnp.mean(widened * widened, axis=-1, keepdims=True) + epsilon)
        * norm_gain
    ).astype(jnp.bfloat16)
    branch = 0.0
    for by in range(n_tp - 1, -1, -1):
        rows_in = rotated(normed, "tp", by) if by else normed
        hidden = squared_relu(jnp.dot(rows_in, up_whole, preferred_element_type=jnp.float32))
        partial = jnp.dot(hidden, down_whole, preferred_element_type=jnp.float32).astype(
            jnp.bfloat16
        )
        if by:
            partial = rotated(partial, "tp", n_tp - by)
        branch = branch + partial.astype(jnp.float32)
    return (widened + rounded(branch).astype(jnp.float32)).astype(jnp.bfloat16)


def fits(mesh, tokens, width, kv_width, model, hidden):
    n_sp, n_tp = mesh.shape["sp"], mesh.shape["tp"]
    block = model // n_sp
    return (
        n_tp == 2
        and n_sp % (n_tp * CORES) == 0
        and n_sp // (n_tp * CORES) >= 3
        and block % LANES == 0
        and kv_width == LANES
        and width % (2 * LANES) == 0
        and tokens % (2 * WINDOW_REACH // 2) == 0
        and (tokens // n_tp) % 32 == 0
        and hidden % (n_tp * 2 * LANES) == 0
    )


def layer_kernel(
    n_z,
    q_hbm, k_hbm, v_hbm, docs_hbm, sinks_hbm, outw_hbm, res_hbm, gain_hbm, up_hbm, down_hbm,
    out_ref,
    up_all, down_all, rows_all, hid_all, outw, res, mixed, q_ref, k_ref, v_ref, docs, docs_prev, docs_flat, sinks, gain_ref,
    k_wide, v_wide, att, oth, psend, precv, own_sum,
    load_sem, halo_send, halo_recv, xs_sem, xr_sem, z_send, z_recv, d_send, d_recv, y_sem,
    g_send, g_recv, p_send, p_recv, own_sem, tail_sem,
):
    sp, y = lax.axis_index("sp"), lax.axis_index("tp")
    n_x, n_y = 2, 2
    z, x, c = sp // (n_x * CORES), lax.rem(sp // CORES, n_x), lax.rem(sp, CORES)
    n_sp = n_z * n_x * CORES
    tokens = q_ref.shape[0]
    rows = res.shape[0]
    half = rows // 2
    model = res.shape[1]
    width = q_ref.shape[1]
    blk = up_hbm.shape[0]
    quarter = up_hbm.shape[1] // n_x
    wide = 2 * blk

    def at(zz, xx, yy, cc):
        return ((zz * n_x + xx) * CORES + cc, yy)

    def remote(src, dst, send, recv, dev):
        return pltpu.make_async_remote_copy(
            src_ref=src, dst_ref=dst, send_sem=send, recv_sem=recv, device_id=dev, device_id_type=MESH
        )

    x_peer, y_peer, c_peer = at(z, 1 - x, y, c), at(z, x, 1 - y, c), at(z, x, y, 1 - c)

    def block(phase, zb, xb, cb):
        if phase == 0:
            first = ((zb * n_x + xb) * CORES + cb) * blk
            return up_all.at[pl.ds(pl.multiple_of(first, blk), blk), :]
        return down_all.at[zb * n_x + xb, :, pl.ds(pl.multiple_of(cb * blk, blk), blk)]

    def own_piece(phase, xq):
        start = pl.multiple_of(xq * quarter, quarter)
        if phase == 0:
            return up_hbm.at[:, pl.ds(start, quarter)]
        return down_hbm.at[pl.ds(start, quarter), :]

    def part_of(ref, h):
        size = ref.shape[0] // 2
        return ref.at[pl.ds(h * size, size), :]

    def x_exchange(phase, h):
        return remote(
            part_of(own_piece(phase, 1 - x), h), part_of(block(phase, z, x, c), h),
            xs_sem.at[phase], xr_sem.at[phase, h], x_peer,
        )

    def own_load(phase):
        return pltpu.make_async_copy(own_piece(phase, x), block(phase, z, x, c), own_sem.at[phase])

    low = jnp.minimum(z, n_z - 1 - z)
    inward = jnp.where(2 * z < n_z, 1, -1)

    def plane(k):
        near = z + jnp.where(lax.rem(k, 2) == 1, inward, -inward) * ((k + 1) // 2)
        far = jnp.where(z < n_z - 1 - z, k, n_z - 1 - k)
        return jnp.where(k <= 2 * low, near, far)

    def place(t):
        zb, b = plane(t // 2), lax.rem(t, 2)
        return zb, b, jnp.where(b == 0, x, 1 - x)

    def to_up(phase, zb, b, xb):
        ref = block(phase, zb, xb, c)
        return remote(ref, ref, z_send.at[phase], z_recv.at[phase, zb, b], at(z + 1, x, y, c))

    def to_down(phase, zb, b, xb):
        ref = block(phase, zb, xb, c)
        return remote(ref, ref, z_send.at[phase], z_recv.at[phase, zb, b], at(z - 1, x, y, c))

    def to_core(phase, zb, b, xb):
        ref = block(phase, zb, xb, c)
        slot = 0 if phase == 0 else 1 + zb * n_x + b
        return remote(ref, ref, d_send.at[phase], d_recv.at[slot], c_peer)

    def to_core_all(phase, less=0):
        ref = up_all.at[pl.ds(0, (2 * n_z - less) * blk), :]
        return remote(ref, ref, d_send.at[phase], d_recv.at[0], c_peer)

    def goes_up(zb):
        return jnp.logical_and(zb <= z, z < n_z - 1)

    def goes_down(zb):
        return jnp.logical_and(zb >= z, z > 0)

    def pass_on(phase, t):
        zb, b, xb = place(t)

        @pl.when(goes_up(zb))
        def _():
            to_up(phase, zb, b, xb).start()

        @pl.when(goes_down(zb))
        def _():
            to_down(phase, zb, b, xb).start()

        to_core(phase, zb, b, xb).start()

    def arrive_x(phase, h):
        x_exchange(phase, h).wait_recv()
        ref = part_of(block(phase, z, 1 - x, c), h)

        @pl.when(z < n_z - 1)
        def _():
            remote(
                ref, ref, z_send.at[phase], z_recv.at[phase, z, 1], at(z + 1, x, y, c)
            ).start()

        @pl.when(z > 0)
        def _():
            remote(
                ref, ref, z_send.at[phase], z_recv.at[phase, z, 1], at(z - 1, x, y, c)
            ).start()

        if h == 1:
            to_core(phase, z, 1, 1 - x).start()

    def arrive(phase, t):
        zb, b, xb = place(t)
        to_up(phase, zb, b, xb).wait_recv()
        pass_on(phase, t)

    last = tokens - WINDOW_REACH
    nxt = (sp + 1, y)

    def halo(i):
        src, dst = (
            (k_hbm.at[pl.ds(last, WINDOW_REACH), :], k_ref.at[pl.ds(0, WINDOW_REACH), :]),
            (v_hbm.at[pl.ds(last, WINDOW_REACH), :], v_ref.at[pl.ds(0, WINDOW_REACH), :]),
            (docs_hbm, docs_prev),
        )[i]
        return remote(src, dst, halo_send.at[i], halo_recv.at[i], nxt)

    own_load(0).start()
    barrier = pltpu.get_barrier_semaphore()
    partners = (
        (True, x_peer), (True, y_peer), (True, at(z, 1 - x, 1 - y, c)), (True, c_peer),
        (z < n_z - 1, at(z + 1, x, y, c)), (z > 0, at(z - 1, x, y, c)),
        (sp < n_sp - 1, nxt), (sp > 0, (sp - 1, y)),
    )
    for here, dev in partners:
        @pl.when(here)
        def _():
            pl.semaphore_signal(barrier, inc=1, device_id=dev, device_id_type=MESH)

    pl.semaphore_wait(barrier, sum(jnp.int32(here) for here, _ in partners))

    @pl.when(sp < n_sp - 1)
    def _():
        for i in range(3):
            halo(i).start()

    loads = [
        pltpu.make_async_copy(q_hbm, q_ref, load_sem.at[0]),
        pltpu.make_async_copy(k_hbm, k_ref.at[pl.ds(WINDOW_REACH, tokens), :], load_sem.at[1]),
        pltpu.make_async_copy(v_hbm, v_ref.at[pl.ds(WINDOW_REACH, tokens), :], load_sem.at[2]),
        pltpu.make_async_copy(outw_hbm, outw, load_sem.at[3]),
        pltpu.make_async_copy(res_hbm, res, load_sem.at[4]),
        pltpu.make_async_copy(gain_hbm, gain_ref, load_sem.at[5]),
        pltpu.make_async_copy(docs_hbm, docs_flat, load_sem.at[6]),
        pltpu.make_async_copy(sinks_hbm, sinks, load_sem.at[7]),
    ]
    own_load(0).wait()

    def begin():
        x_exchange(0, 0).start()
        pass_on(0, 0)
        x_exchange(0, 1).start()

    @pl.when(c == 1)
    def _():
        begin()

    for load in loads:
        load.start()
    own_load(1).start()

    @pl.when(sp == 0)
    def _():
        k_ref[pl.ds(0, WINDOW_REACH), :] = jnp.zeros((WINDOW_REACH, LANES), jnp.bfloat16)
        v_ref[pl.ds(0, WINDOW_REACH), :] = jnp.zeros((WINDOW_REACH, LANES), jnp.bfloat16)
        docs_prev[...] = jnp.full(docs_prev.shape, -1, jnp.int32)

    for load in loads[:3] + loads[6:]:
        load.wait()

    @pl.when(sp > 0)
    def _():
        for i in range(3):
            halo(i).wait_recv()

    docs[0, 0] = docs_prev[last:]
    for i in range(tokens // LANES):
        docs[i + 1, 0] = docs_flat[i * LANES : (i + 1) * LANES]
    @pl.when(c == 0)
    def _():
        begin()

    heads = width // HEAD_SIZE
    kv_heads = LANES // HEAD_SIZE
    group = heads // kv_heads
    lane_in = lax.broadcasted_iota(jnp.int32, (LANES, LANES), 0)
    lane_out = lax.broadcasted_iota(jnp.int32, (LANES, LANES), 1)
    for g in range(kv_heads):
        for par in range(2):
            pick = (lane_in - g * HEAD_SIZE == lane_out - par * HEAD_SIZE) & (
                lane_out // HEAD_SIZE == par
            )
            pick = pick.astype(jnp.float32).astype(jnp.bfloat16)
            for raw, spread in ((k_ref, k_wide), (v_ref, v_wide)):
                spread[g * 2 + par] = jnp.dot(
                    raw[...], pick, preferred_element_type=jnp.float32
                ).astype(jnp.bfloat16)

    row_i = lax.broadcasted_iota(jnp.int32, (WINDOW_REACH, 2 * WINDOW_REACH), 0)
    col_i = lax.broadcasted_iota(jnp.int32, (WINDOW_REACH, 2 * WINDOW_REACH), 1)
    near = (col_i > row_i) & (col_i <= row_i + WINDOW_REACH)

    def attend(n, carry):
        start = pl.multiple_of(n * WINDOW_REACH, WINDOW_REACH)
        early = jnp.broadcast_to(docs[n], (WINDOW_REACH, LANES))
        late = jnp.broadcast_to(docs[n + 1], (WINDOW_REACH, LANES))
        mine = late.T
        same = jnp.concatenate([early == mine, late == mine], axis=1)
        visible = near & same
        for j in range(width // LANES):
            total_out = None
            g = (2 * j) // group
            q_blk = q_ref[pl.ds(start, WINDOW_REACH), j * LANES : (j + 1) * LANES]
            for par in range(2):
                head = 2 * j + par
                keys = k_wide[g * 2 + par, pl.ds(start, 2 * WINDOW_REACH), :]
                vals = v_wide[g * 2 + par, pl.ds(start, 2 * WINDOW_REACH), :]
                scores = lax.dot_general(
                    q_blk, keys, (((1,), (1,)), ((), ())), preferred_element_type=jnp.float32
                ) * HEAD_SIZE ** (-0.5)
                scores = jnp.where(visible, scores, masked_score)
                sink = sinks[head]
                top = jnp.maximum(jnp.max(scores, axis=1, keepdims=True), sink)
                exponent = jnp.where(visible, jnp.exp(scores - top), 0.0)
                total = jnp.exp(sink - top) + jnp.sum(exponent, axis=1, keepdims=True)
                shares = (exponent * (1.0 / total)).astype(jnp.bfloat16)
                part = jnp.dot(shares, vals, preferred_element_type=jnp.float32)
                total_out = part if total_out is None else total_out + part
            att[pl.ds(start, WINDOW_REACH), j * LANES : (j + 1) * LANES] = total_out.astype(
                jnp.bfloat16
            )

        @pl.when(n == steps // 2 + 1)
        def _():
            arrive_x(0, 0)

        return carry

    steps = tokens // WINDOW_REACH
    lax.fori_loop(0, steps, attend, 0)

    mine_at = pl.multiple_of(y * rows, rows)
    theirs_at = pl.multiple_of((1 - y) * rows, rows)
    swap = remote(att.at[pl.ds(theirs_at, rows), :], oth, y_sem.at[0], y_sem.at[1], y_peer)
    swap.start()
    for h in range(2):
        x_exchange(1, h).start()
    arrive_x(0, 1)
    arrive(0, 2)
    for load in loads[3:6]:
        load.wait()
    swap.wait_recv()

    me_p = x * n_y + y
    x_p, y_p, d_p = (1 - x) * n_y + y, x * n_y + 1 - y, (1 - x) * n_y + 1 - y
    chunk = 2 * wide

    def row_part(p, h):
        return rows_all.at[pl.ds(pl.multiple_of(p * rows + h * half, half), half), :]

    def give(p, h, way):
        ref = row_part(p, h)
        return remote(ref, ref, g_send.at[0], g_recv.at[p * 2 + h], x_peer if way == 0 else y_peer)

    for h in range(2):
        own_rows = pl.ds(pl.multiple_of(mine_at + h * half, half), half)

        def project(n, square):
            cols = pl.ds(pl.multiple_of(n * chunk, chunk), chunk)
            acc = jnp.dot(
                att[own_rows, :], outw[pl.ds(pl.multiple_of(y * width, width), width), cols],
                preferred_element_type=jnp.float32,
            ) + jnp.dot(
                oth[h * half : (h + 1) * half, :],
                outw[pl.ds(pl.multiple_of((1 - y) * width, width), width), cols],
                preferred_element_type=jnp.float32,
            )
            sums = res[h * half : (h + 1) * half, cols].astype(jnp.float32) + acc.astype(
                jnp.bfloat16
            ).astype(jnp.float32)
            sums = sums.astype(jnp.bfloat16)
            mixed[h * half : (h + 1) * half, cols] = sums
            sums = sums.astype(jnp.float32)
            return square + jnp.sum(sums * sums, axis=1, keepdims=True)

        square = lax.fori_loop(0, model // chunk, project, jnp.zeros((half, 1), jnp.float32))
        scale = lax.rsqrt(square * (1.0 / model) + epsilon)

        def normalise(n, carry):
            cols = pl.ds(pl.multiple_of(n * chunk, chunk), chunk)
            wide_rows = mixed[h * half : (h + 1) * half, cols].astype(jnp.float32)
            rows_all[pl.ds(pl.multiple_of(me_p * rows + h * half, half), half), cols] = (
                wide_rows * scale * gain_ref[:, cols]
            ).astype(jnp.bfloat16)
            return carry

        lax.fori_loop(0, model // chunk, normalise, 0)
        give(me_p, h, 0).start()
        give(me_p, h, 1).start()

    arrive(0, 3)
    n_items = 2 * n_z

    def more(first, until):
        for t in range(first, min(until, n_items)):
            arrive(0, t)

    more(4, 6)
    give(x_p, 0, 0).wait_recv()
    give(x_p, 0, 1).start()
    more(6, 7)
    give(y_p, 1, 1).wait_recv()
    give(y_p, 1, 0).start()
    more(7, n_items)

    own_load(1).wait()
    pass_on(1, 0)
    for h in range(2):
        arrive_x(1, h)

    give(x_p, 1, 0).wait_recv()
    give(y_p, 0, 1).wait_recv()
    give(d_p, 0, 1).wait_recv()
    give(d_p, 1, 0).wait_recv()

    to_core_all(0).wait_recv()
    tall = 2 * rows

    def up_step(i, carry):
        r = pl.ds(pl.multiple_of((i // (quarter // chunk)) * tall, tall), tall)
        f = pl.ds(pl.multiple_of(lax.rem(i, quarter // chunk) * chunk, chunk), chunk)
        before = jnp.dot(rows_all[r, :], up_all[:, f], preferred_element_type=jnp.float32)
        before = jnp.maximum(before, 0.0)
        hid_all[r, f] = (before * before).astype(jnp.bfloat16)
        return carry

    lax.fori_loop(0, 2 * (quarter // chunk), up_step, 0)

    def lanes(ref, h):
        if h is None:
            return ref
        cut = pl.ds(h * blk, blk)
        return ref.at[:, cut] if len(ref.shape) == 2 else ref.at[:, :, cut]

    def partial_slot(j, h):
        return 2 * n_z + lax.rem(j, n_x) if h == 0 else j

    def way(s):
        return jnp.where(s >= 2, 1 - x, x), jnp.where(lax.rem(s, 2) == 1, 1 - y, y)

    def partial_copy(j, s, h=None):
        px, py = way(s)
        return remote(
            lanes(psend.at[j, s - 1], h), lanes(precv.at[j, s - 1], h),
            p_send.at[0], p_recv.at[partial_slot(j, h)], at(z, px, py, c),
        )

    def partials(j, h=None):
        return remote(
            lanes(psend.at[j], h), lanes(precv.at[j], h),
            p_send.at[0], p_recv.at[partial_slot(j, h)], x_peer,
        )

    def pair_of(t):
        zb, b, xb = place(t)
        return zb * n_x + xb

    def combine(t, h=None):
        j = pair_of(t)
        total = lanes(own_sum.at[j], h)[...]
        partials(j, h).wait_recv()
        for s in (1, 2, 3):
            total = total + lanes(precv.at[j, s - 1], h)[...].astype(jnp.float32)
        size = wide if h is None else blk
        cols = pl.ds(pl.multiple_of(j * wide + (h or 0) * blk, blk), size)
        out_ref[:, cols] = (
            mixed[:, cols].astype(jnp.float32) + total.astype(jnp.bfloat16).astype(jnp.float32)
        ).astype(jnp.bfloat16)

    def pieces(j, h=None):
        def piece(i, carry):
            s = jnp.where(i == 0, 1, jnp.where(i == 1, 3, jnp.where(i == 2, 2, 0)))
            px, py = way(s)
            first = pl.multiple_of((px * n_y + py) * rows, rows)
            part = jnp.dot(
                hid_all[pl.ds(first, rows), :], lanes(down_all.at[j], h)[...],
                preferred_element_type=jnp.float32,
            )

            @pl.when(s > 0)
            def _():
                lanes(psend.at[j, s - 1], h)[...] = part.astype(jnp.bfloat16)
                partial_copy(j, s, h).start()

            @pl.when(s == 0)
            def _():
                lanes(own_sum.at[j], h)[...] = part

            return carry

        lax.fori_loop(0, n_x * n_y, piece, 0)

    lag = 4
    n_whole = n_items - 2

    def line_sent(phase):
        for here in range(n_z):
            blocks = 2 * (here + 1) * (here < n_z - 1) + 2 * (n_z - here) * (here > 0)

            @pl.when(z == here)
            def _():
                if phase == 0:
                    ref = up_all.at[pl.ds(0, blocks * blk), :]
                else:
                    ref = down_all.at[pl.ds(0, blocks // 2)]
                remote(ref, ref, z_send.at[phase], z_recv.at[phase, 0, 0], x_peer).wait_send()

    @pl.when(sp < n_sp - 1)
    def _():
        for i in range(3):
            halo(i).wait_send()

    swap.wait_send()
    for phase in range(2):
        whole = block(phase, z, x, c)
        remote(whole, whole, xs_sem.at[phase], xr_sem.at[phase, 0], x_peer).wait_send()

    def down_step(t, carry):
        @pl.when(t >= 2)
        def _():
            arrive(1, t)

        zb, b, xb = place(t)
        to_core(1, zb, b, xb).wait_recv()
        pieces(pair_of(t))

        @pl.when(t >= lag)
        def _():
            combine(t - lag)

        return carry

    lax.fori_loop(0, n_whole, down_step, 0)

    at_end = jnp.logical_or(z == 0, z == n_z - 1)
    z_last, _, x_last = place(n_items - 1)
    last_slot = 1 + z_last * n_x + 1

    def tail_half(part, send, recv, dev):
        ref = part_of(block(1, z_last, x_last, 0), part)
        return remote(ref, ref, send, recv, dev)

    def tail_first():
        tail_half(0, tail_sem.at[0], z_recv.at[1, z_last, 1], c_peer).wait_recv()
        tail_half(0, tail_sem.at[0], d_recv.at[last_slot], c_peer).start()

    def tail_second():
        tail_half(1, tail_sem.at[0], tail_sem.at[1], c_peer).wait_recv()
        tail_half(1, tail_sem.at[0], tail_sem.at[1], c_peer).start()
        tail_half(0, tail_sem.at[0], d_recv.at[last_slot], c_peer).wait_recv()

    def tail_forward():
        to_up(1, z_last, 1, x_last).wait_recv()
        for outer, towards in ((n_z - 1, 1), (0, -1)):
            @pl.when(jnp.logical_and(z + towards == outer, (z_last - z) * towards < 0))
            def _():
                tail_half(0, z_send.at[1], z_recv.at[1, z_last, 1], at(z + towards, x, y, 0)).start()
                tail_half(1, z_send.at[1], tail_sem.at[1], at(z + towards, x, y, 1)).start()

        to_core(1, z_last, 1, x_last).start()

    def last_step(t, carry):
        for h in (1, 0):
            halved = jnp.logical_and(t == n_items - 1, at_end)
            if h == 1:
                @pl.when(jnp.logical_and(halved, c == 0))
                def _():
                    tail_first()

                own, other = c == 1, c == 0
            else:
                final = jnp.logical_and(t == n_items - 1, jnp.logical_not(at_end))

                @pl.when(jnp.logical_and(halved, c == 0))
                def _():
                    tail_half(1, tail_sem.at[0], tail_sem.at[1], c_peer).wait_recv()

                @pl.when(jnp.logical_and(halved, c == 1))
                def _():
                    tail_second()

                @pl.when(jnp.logical_and(final, c == 0))
                def _():
                    tail_forward()

                own = jnp.logical_and(c == 0, t < n_items - 1)
                other = jnp.logical_and(c == 1, jnp.logical_not(halved))

            @pl.when(own)
            def _():
                arrive(1, t)

            @pl.when(other)
            def _():
                zb, b, xb = place(t)
                to_core(1, zb, b, xb).wait_recv()

            pieces(pair_of(t), h)
            done = n_whole - lag + 2 * (t - n_whole) + 1 - h

            @pl.when(done < n_whole - 1)
            def _():
                combine(done)

        return carry

    line_sent(0)
    lax.fori_loop(n_whole, n_items, last_step, 0)
    given = rows_all.at[pl.ds(0, 3 * rows), :]
    remote(given, given, g_send.at[0], g_recv.at[0], x_peer).wait_send()
    line_sent(1)
    to_core_all(0).wait_send()

    @pl.when(jnp.logical_or(jnp.logical_not(at_end), c == 1))
    def _():
        to_core_all(1).wait_send()

    @pl.when(jnp.logical_and(at_end, c == 0))
    def _():
        to_core_all(1, 1).wait_send()

    @pl.when(at_end)
    def _():
        tail_half(0, tail_sem.at[0], tail_sem.at[1], c_peer).wait_send()

    for t in range(n_whole - 1, n_items):
        for h in (None,) if t < n_whole else (1, 0):
            combine(jnp.int32(t), h)

    remote(psend, precv, p_send.at[0], p_recv.at[0], x_peer).wait_send()


def kernel_body(
    n_z, queries, keys, values, documents, sinks, out_weight, residual, norm_gain, up_weight, down_weight
):
    tokens, width = queries.shape
    rows, model = residual.shape
    blk, hidden = up_weight.shape
    quarter = hidden // 2
    group = 4 * rows
    pairs = 2 * n_z
    bf16, f32 = jnp.bfloat16, jnp.float32
    hbm = pl.BlockSpec(memory_space=pl.ANY)
    dma = pltpu.SemaphoreType.DMA
    return pl.pallas_call(
        functools.partial(layer_kernel, n_z),
        out_shape=pltpu.VMEM((rows, model), bf16),
        in_specs=[hbm] * 10,
        out_specs=pl.BlockSpec(memory_space=pltpu.VMEM),
        scratch_shapes=[
            pltpu.VMEM((model, quarter), bf16),
            pltpu.VMEM((pairs, quarter, 2 * blk), bf16),
            pltpu.VMEM((group, model), bf16),
            pltpu.VMEM((group, quarter), bf16),
            pltpu.VMEM(out_weight.shape, bf16),
            pltpu.VMEM((rows, model), bf16),
            pltpu.VMEM((rows, model), bf16),
            pltpu.VMEM((tokens, width), bf16),
            pltpu.VMEM((tokens + WINDOW_REACH, LANES), bf16),
            pltpu.VMEM((tokens + WINDOW_REACH, LANES), bf16),
            pltpu.VMEM((tokens // LANES + 1, 1, LANES), jnp.int32),
            pltpu.VMEM((tokens,), jnp.int32),
            pltpu.VMEM((tokens,), jnp.int32),
            pltpu.SMEM(sinks.shape, f32),
            pltpu.VMEM((1, model), f32),
            pltpu.VMEM((4, tokens + WINDOW_REACH, LANES), bf16),
            pltpu.VMEM((4, tokens + WINDOW_REACH, LANES), bf16),
            pltpu.VMEM((tokens, width), bf16),
            pltpu.VMEM((rows, width), bf16),
            pltpu.VMEM((pairs, 3, rows, 2 * blk), bf16),
            pltpu.VMEM((pairs, 3, rows, 2 * blk), bf16),
            pltpu.VMEM((pairs, rows, 2 * blk), f32),
            dma((8,)), dma((3,)), dma((3,)), dma((2,)), dma((2, 2)), dma((2,)), dma((2, n_z, 2)),
            dma((2,)), dma((1 + 2 * n_z,)), dma((2,)), dma((1,)), dma((8,)),
            dma((1,)), dma((pairs + 2,)), dma((2,)), dma((2,)),
        ],
        compiler_params=pltpu.CompilerParams(collective_id=0, has_side_effects=True, vmem_limit_bytes=60 << 20),
    )(
        queries, keys, values, documents, sinks, out_weight,
        residual, norm_gain.reshape(1, model), up_weight, down_weight,
    )


def body(n_z, mesh, *arrays):
    queries, keys, up_weight, residual = arrays[0], arrays[1], arrays[8], arrays[6]
    if fits(mesh, *queries.shape, keys.shape[1], residual.shape[1], up_weight.shape[1]):
        return kernel_body(n_z, *arrays)
    return gathered_body(*arrays)


def solution(mesh):
    in_specs = (
        P("sp", "tp"),
        P("sp", "tp"),
        P("sp", "tp"),
        P("sp"),
        P("tp"),
        P(),
        P(("sp", "tp"), None),
        P(),
        P("sp", "tp"),
        P("tp", "sp"),
    )
    out_specs = P(("sp", "tp"), None)
    n_z = mesh.shape["sp"] // (CORES * mesh.shape["tp"])
    return jax.shard_map(
        functools.partial(body, n_z, mesh), mesh=mesh, in_specs=in_specs, out_specs=out_specs, check_vma=False
    )
```
